32 devices in a mesh: ep: 32 (over z, y, x, core).
Axes of the slice: x: 2, y: 2, z: 4, core: 2. Of those that a mesh axis runs over, the one named last changes fastest.
Arguments:
- tokens: bfloat16 [512, 1024], P('ep'), may hold values from -6 to 6
- lengths: int32 [512], P('ep'), may hold values from 1 to 8191
- cache_keys: bfloat16 [512, 128, 512], P('ep'), may hold values from -6 to 6
- cache_values: bfloat16 [512, 128, 1024], P('ep'), may hold values from -6 to 6
- retention_state: float32 [512, 4, 128, 256], P('ep'), may hold values from -24 to 24
- mix_gain: float32 [1024], replicated, may hold values from 0.1 to 1.9
- query_weight: bfloat16 [1024, 512], replicated, may hold values from -0.1875 to 0.1875
- key_weight: bfloat16 [1024, 512], replicated, may hold values from -0.1875 to 0.1875
- value_weight: bfloat16 [1024, 1024], replicated, may hold values from -0.1875 to 0.1875
- out_weight: bfloat16 [1024, 1024], replicated, may hold values from -0.1875 to 0.1875
- ffn_gain: float32 [1024], replicated, may hold values from 0.1 to 1.9
- routes: int32 [512, 6], P('ep'), may hold values from 0 to 31, all different within a row; in each aligned block of 16 rows (0 to 15, 16 to 31, ...) at most 8 rows name the same one
- route_scores: float32 [512, 6], P('ep'), may hold values from 0.05 to 1
- expert_gate: bfloat16 [32, 1024, 256], P('ep'), may hold values from -0.1875 to 0.1875
- expert_up: bfloat16 [32, 1024, 256], P('ep'), may hold values from -0.1875 to 0.1875
- expert_down: bfloat16 [32, 256, 1024], P('ep'), may hold values from -0.375 to 0.375
- shared_gate: bfloat16 [1024, 256], replicated, may hold values from -0.1875 to 0.1875
- shared_up: bfloat16 [1024, 256], replicated, may hold values from -0.1875 to 0.1875
- shared_down: bfloat16 [256, 1024], replicated, may hold values from -0.375 to 0.375
- dense_gate: bfloat16 [4096, 1024], P('ep'), may hold values from -0.1875 to 0.1875
- dense_up: bfloat16 [4096, 1024], P('ep'), may hold values from -0.1875 to 0.1875
- dense_down: bfloat16 [4096, 1024], P('ep'), may hold values from -0.09375 to 0.09375
- dense_mix: float32 [1024], replicated, may hold values from -3 to 3
Outputs:
- layer_out: bfloat16 [512, 1024], P('ep')
- new_keys: bfloat16 [512, 512], P('ep')
- new_values: bfloat16 [512, 1024], P('ep')
The draws below stay inside these ranges and needn't reach their ends.
Inputs may be any that keep to these rules, and one draw needn't show every extreme that they name: `routes`: each row names 6 different experts; among the rows of one device no expert is named more than 8 times.
All inputs are finite; a program needn't handle non-finite values.
Results may differ from the reference program's by a relative error of at most 0.012.
Values may be sent and summed in bfloat16 or wider, within the bound.
A program may use at most 128 MiB of HBM per device.

```python
import math
import jax
import jax.numpy as jnp
import numpy as np
from jax import lax

D = 1024
HEADS = 4
DK = 128
DV = 256
BLOCK = 128
SEQ_DEV = 16
SEQS = 512
EXPERTS = 32
TOP_K = 6
CAP = 8
EH = 256
SH = 256
DENSE_FF = 4096
N_EP = 32


def plant(values, stream_key, smallest, top_value):
    dims = values.shape
    spot = [jax.random.randint(jax.random.fold_in(stream_key, axis), (), 0, dims[axis]) for axis in range(len(dims))]
    values = values.at[tuple(spot)].set(smallest)
    longest = dims.index(max(dims))
    spot[longest] = (spot[longest] + 1) % dims[longest]
    return values.at[tuple(spot)].set(top_value)


def shard_levels(rng, dims, shards, low, high):
    factor_of = 1.0
    for axis_at, shards_of in shards:
        heights = jax.random.uniform(jax.random.fold_in(jax.random.fold_in(rng, 6), axis_at), (shards_of,), jnp.float32, low / len(shards), high / len(shards))
        factor_of = factor_of * jnp.repeat(jnp.exp(heights), dims[axis_at] // shards_of).reshape((-1,) + (1,) * (len(dims) - 1 - axis_at))
    return factor_of


def routed_block(key, own, number, rows, count, top, reach, slope):
    sequence = jax.random.permutation(key, count)
    crowded, common = portions_of(count, rows * top, reach, slope, True), portions_of(count, rows * top, reach, slope, False)
    places = jnp.arange(count)

    def named(tallies, offset_by):
        used = int((tallies > 0).sum())
        fixed = max(1, used // 4)
        passed = fixed + (places - fixed + offset_by * (used - fixed)) % max(1, count - fixed)
        return jnp.zeros((count,), jnp.int32).at[sequence[jnp.where(places < fixed, places, passed)]].set(jnp.asarray(tallies, jnp.int32))

    tallies = jnp.where(number % 4 == 0, named(crowded, number // 4), named(common, number - number // 4 - 1))
    mixed = jax.random.permutation(jax.random.fold_in(own, 3), count)
    donor, receiver = mixed[0:count // 2 * 2:2], mixed[1:count // 2 * 2:2]
    room = jnp.minimum(tallies[donor] - 1, reach - tallies[receiver]) // 2
    room = jnp.where((donor == sequence[0]) | (receiver == sequence[0]) | (tallies[receiver] == 0), 0, jnp.maximum(room, 0))
    passed = jax.random.randint(jax.random.fold_in(own, 4), (count // 2,), 0, 1 << 20) % (room + 1)
    tallies = tallies.at[donor].add(-passed).at[receiver].add(passed)
    members = jnp.searchsorted(jnp.cumsum(tallies), jnp.arange(rows * top), side="right").astype(jnp.int32)
    grid = members.reshape(top, rows).T
    grid = grid[jax.random.permutation(jax.random.fold_in(own, 1), rows)]
    offset_by = jax.random.randint(jax.random.fold_in(own, 2), (rows, 1), 0, top)
    return jnp.take_along_axis(grid, (jnp.arange(top)[None, :] + offset_by) % top, axis=1)


def portions_of(amount, total, limit, slope, full):
    portions = [(1 << 20) // math.isqrt(grade ** slope) + 1 for grade in range(1, amount + 1)]
    largest = limit if full else min(limit, max(-(-total // amount), total * portions[0] // sum(portions)))
    least = 1 if total - largest >= amount - 1 else 0
    counts, surplus = [largest] + [least] * (amount - 1), total - largest - least * (amount - 1)
    while surplus > 0:
        free = [i for i in range(1, amount) if counts[i] < largest] or [i for i in range(1, amount) if counts[i] < limit]
        pool, budget = sum([portions[i] for i in free]), surplus
        for i in free:
            addition = min(limit - counts[i], max(1, budget * portions[i] // pool), surplus)
            counts[i] = counts[i] + addition
            surplus = surplus - addition
    return np.array(counts)


def gaussian(own_key, dims, deviation, reach, shards=(), held_as=jnp.bfloat16):
    result = deviation * jax.random.normal(own_key, dims, jnp.float32)
    if shards:
        result = result * shard_levels(own_key, dims, shards, -0.22, 0.18)
    return jnp.clip(result, -reach, reach).astype(held_as)


def setup_inputs(seed: int = 0) -> dict:
    key_of = jax.random.split(jax.random.key(seed), 24)
    tokens = gaussian(key_of[0], (SEQS, D), 1.0, 6.0, ((0, 32),))
    lengths = plant(jax.random.randint(key_of[1], (SEQS,), 1, 8192), jax.random.fold_in(key_of[1], 1), 1, 8191).astype(jnp.int32)
    cache_keys = gaussian(key_of[2], (SEQS, BLOCK, HEADS * DK), 1.0, 6.0, ((0, 32),))
    cache_values = gaussian(key_of[3], (SEQS, BLOCK, HEADS * DV), 1.0, 6.0, ((0, 32),))
    retention_state = gaussian(key_of[4], (SEQS, HEADS, DK, DV), 4.0, 24.0, ((0, 32),), jnp.float32)
    mix_gain = jnp.clip(1.0 + 0.18 * jax.random.normal(key_of[5], (D,), jnp.float32), 0.1, 1.9)
    query_weight = gaussian(key_of[6], (D, HEADS * DK), D ** -0.5, 0.1875)
    key_weight = gaussian(key_of[7], (D, HEADS * DK), D ** -0.5, 0.1875)
    value_weight = gaussian(key_of[8], (D, HEADS * DV), D ** -0.5, 0.1875)
    out_weight = gaussian(key_of[9], (HEADS * DV, D), (HEADS * DV) ** -0.5, 0.1875)
    ffn_gain = jnp.clip(1.0 + 0.18 * jax.random.normal(key_of[10], (D,), jnp.float32), 0.1, 1.9)
    routes_keys = jax.random.split(jax.random.fold_in(key_of[11], 1), SEQS // SEQ_DEV)
    routes_turns = jax.random.permutation(jax.random.fold_in(key_of[11], 3), SEQS // SEQ_DEV)
    routes = jax.vmap(lambda own, number: routed_block(jax.random.fold_in(key_of[11], 2), own, number, SEQ_DEV, EXPERTS, TOP_K, CAP, 1))(routes_keys, routes_turns).reshape((SEQS, TOP_K))
    route_scores = jnp.clip(0.05 + 0.95 * jax.random.uniform(key_of[12], (SEQS, TOP_K), jnp.float32) ** shard_levels(key_of[12], (SEQS, TOP_K), ((0, 32),), -0.2, 0.2), 0.05, 1.0)
    expert_gate = gaussian(key_of[13], (EXPERTS, D, EH), D ** -0.5, 0.1875, ((0, 32),))
    expert_up = gaussian(key_of[14], (EXPERTS, D, EH), D ** -0.5, 0.1875, ((0, 32),))
    expert_down = gaussian(key_of[15], (EXPERTS, EH, D), EH ** -0.5, 0.375, ((0, 32),))
    shared_gate = gaussian(key_of[16], (D, SH), D ** -0.5, 0.1875)
    shared_up = gaussian(key_of[17], (D, SH), D ** -0.5, 0.1875)
    shared_down = gaussian(key_of[18], (SH, D), SH ** -0.5, 0.375)
    dense_gate = gaussian(key_of[19], (DENSE_FF, D), D ** -0.5, 0.1875, ((0, 32),))
    dense_up = gaussian(key_of[20], (DENSE_FF, D), D ** -0.5, 0.1875, ((0, 32),))
    dense_down = gaussian(key_of[21], (DENSE_FF, D), DENSE_FF ** -0.5, 0.09375, ((0, 32),))
    dense_mix = jnp.clip(jax.random.uniform(key_of[22], (D,), jnp.float32, -3.0, 3.0), -3.0, 3.0)
    return {"tokens": tokens, "lengths": lengths, "cache_keys": cache_keys, "cache_values": cache_values, "retention_state": retention_state, "mix_gain": mix_gain, "query_weight": query_weight, "key_weight": key_weight, "value_weight": value_weight, "out_weight": out_weight, "ffn_gain": ffn_gain, "routes": routes, "route_scores": route_scores, "expert_gate": expert_gate, "expert_up": expert_up, "expert_down": expert_down, "shared_gate": shared_gate, "shared_up": shared_up, "shared_down": shared_down, "dense_gate": dense_gate, "dense_up": dense_up, "dense_down": dense_down, "dense_mix": dense_mix}


eps = 1e-06
route_scale = 2.5
rope_base = 10000.0

def normed(values):
    return values * lax.rsqrt(lax.optimization_barrier(jnp.mean(values * values, axis=-1, keepdims=True)) + eps)

def log_decay(head_count):
    return jnp.log1p(-jnp.exp2(-5.0 - jnp.arange(head_count, dtype=jnp.float32)))

def rotate(values, positions):
    half_size = values.shape[-1] // 2
    inverse = rope_base ** (-jnp.arange(half_size, dtype=jnp.float32) / half_size)
    angles = positions.astype(jnp.float32)[:, None, None] * inverse[None, None, :]
    cosine = jnp.cos(angles)
    sine_part = jnp.sin(angles)
    first_half = values[..., :half_size]
    second = values[..., half_size:]
    return jnp.concatenate([first_half * cosine - second * sine_part, first_half * sine_part + second * cosine], axis=-1)

def swiglu(inputs, w_gate, w_up, w_down):
    gate_part = jnp.dot(inputs, w_gate, preferred_element_type=jnp.float32)
    up_part = jnp.dot(inputs, w_up, preferred_element_type=jnp.float32)
    hidden = (jax.nn.silu(gate_part) * up_part).astype(jnp.bfloat16)
    return jnp.dot(hidden, w_down, preferred_element_type=jnp.float32)

def retain(tokens, lengths, mix_gain, w_query, w_key, w_value, w_out, cache_keys, cache_values, carry_state):
    seq_count, head_count, key_size, value_size = carry_state.shape
    block_size = cache_keys.shape[1]
    widened = tokens.astype(jnp.float32)
    normal_in = (normed(widened) * mix_gain).astype(jnp.bfloat16)
    raw_query = jnp.dot(normal_in, w_query, preferred_element_type=jnp.float32).reshape(seq_count, head_count, key_size)
    raw_key = jnp.dot(normal_in, w_key, preferred_element_type=jnp.float32).reshape(seq_count, head_count, key_size)
    raw_value = jnp.dot(normal_in, w_value, preferred_element_type=jnp.float32).reshape(seq_count, head_count, value_size)
    queries = (rotate(raw_query, lengths) * key_size ** (-0.5)).astype(jnp.bfloat16)
    new_keys = rotate(raw_key, lengths).astype(jnp.bfloat16)
    new_values = raw_value.astype(jnp.bfloat16)
    filled = lengths % block_size
    decay_rate = log_decay(head_count)
    places = jnp.arange(block_size, dtype=jnp.int32)
    stored_keys = cache_keys.reshape(seq_count, block_size, head_count, key_size)
    stored_values = cache_values.reshape(seq_count, block_size, head_count, value_size)
    scores = jnp.einsum('shd,sjhd->shj', queries.astype(jnp.float32), stored_keys.astype(jnp.float32))
    distance = jnp.maximum(filled[:, None] - places[None, :], 0).astype(jnp.float32)
    live_mask = places[None, :] < filled[:, None]
    weighted = jnp.where(live_mask[:, None, :], scores * jnp.exp(distance[:, None, :] * decay_rate[None, :, None]), 0.0).astype(jnp.bfloat16)
    own_weight = lax.optimization_barrier(jnp.sum(queries.astype(jnp.float32) * new_keys.astype(jnp.float32), axis=-1)).astype(jnp.bfloat16)
    inside = jnp.einsum('shj,sjhe->she', weighted.astype(jnp.float32), stored_values.astype(jnp.float32))
    inside = inside + own_weight.astype(jnp.float32)[:, :, None] * new_values.astype(jnp.float32)
    carried = jnp.einsum('shd,shde->she', queries.astype(jnp.float32), carry_state, precision=lax.Precision.HIGHEST)
    carried = carried * jnp.exp((filled.astype(jnp.float32)[:, None] + 1.0) * decay_rate[None, :])[:, :, None]
    headed = normed(inside + carried).astype(jnp.bfloat16).reshape(seq_count, head_count * value_size)
    mixer_out = jnp.dot(headed, w_out, preferred_element_type=jnp.float32)
    residual = widened + normed(mixer_out)
    return (residual, new_keys.reshape(seq_count, head_count * key_size), new_values.reshape(seq_count, head_count * value_size))

def reference(tokens, lengths, cache_keys, cache_values, retention_state, mix_gain, query_weight, key_weight, value_weight, out_weight, ffn_gain, routes, route_scores, expert_gate, expert_up, expert_down, shared_gate, shared_up, shared_down, dense_gate, dense_up, dense_down, dense_mix):
    residual, new_keys, new_values = retain(tokens, lengths, mix_gain, query_weight, key_weight, value_weight, out_weight, cache_keys, cache_values, retention_state)
    normal_ffn = (normed(residual) * ffn_gain).astype(jnp.bfloat16)
    shared_out = swiglu(normal_ffn, shared_gate, shared_up, shared_down)
    dense_gate_part = jnp.dot(normal_ffn, dense_gate.T, preferred_element_type=jnp.float32)
    dense_up_part = jnp.dot(normal_ffn, dense_up.T, preferred_element_type=jnp.float32)
    dense_hidden = (jax.nn.silu(dense_gate_part) * dense_up_part).astype(jnp.bfloat16)
    dense_out = jnp.dot(dense_hidden, dense_down, preferred_element_type=jnp.float32)
    route_weight = route_scores / lax.optimization_barrier(jnp.sum(route_scores, axis=-1, keepdims=True)) * route_scale
    flat_routes = routes.reshape(-1)
    flat_weight = route_weight.reshape(-1)
    most_rows = N_EP * CAP
    slot_rank = jnp.arange(most_rows, dtype=jnp.int32)

    def one_expert(running, expert_id):
        hits = flat_routes == expert_id
        hit_count = jnp.sum(hits.astype(jnp.int32))
        picked = jnp.nonzero(hits, size=most_rows, fill_value=0)[0].astype(jnp.int32)
        is_valid = slot_rank < hit_count
        row_ids = picked // TOP_K
        outputs = swiglu(normal_ffn[row_ids], expert_gate[expert_id], expert_up[expert_id], expert_down[expert_id]).astype(jnp.bfloat16)
        added = jnp.where(is_valid[:, None], outputs.astype(jnp.float32) * flat_weight[picked][:, None], 0.0)
        return (running.at[row_ids].add(added), None)
    routed, _ = lax.scan(one_expert, jnp.zeros(residual.shape, jnp.float32), jnp.arange(EXPERTS, dtype=jnp.int32))
    combined = shared_out + routed + jax.nn.sigmoid(dense_mix) * dense_out
    layer_out = (residual + normed(combined)).astype(jnp.bfloat16)
    return (layer_out, new_keys, new_values)
```

```python
import functools
import math

import jax
import jax.numpy as jnp
from jax import lax
from jax.experimental import pallas as pl
from jax.experimental.pallas import tpu as pltpu
from jax.sharding import PartitionSpec as P

eps = 1e-06
route_scale = 2.5
rope_base = 10000.0

f32 = jnp.float32
bf16 = jnp.bfloat16
lanes = 128


def inverse_rms(values):
    return lax.rsqrt(jnp.mean(values * values, axis=-1, keepdims=True) + eps)


def mm(a, b):
    return lax.dot_general(a, b, (((1,), (0,)), ((), ())), preferred_element_type=f32)


def mm_t(a, b):
    return lax.dot_general(a, b, (((1,), (1,)), ((), ())), preferred_element_type=f32)


def cos_sin(angles):
    turn = jnp.floor(angles * (2.0 / math.pi) + 0.5)
    r = angles - turn * 1.5703125
    r = r - turn * 4.837512969970703125e-4
    r = r - turn * 7.54978995489188216e-8
    z = r * r
    sine = ((-1.9515295891e-4 * z + 8.3321608736e-3) * z - 1.6666654611e-1) * z * r + r
    cosine = ((2.443315711809948e-5 * z - 1.388731625493765e-3) * z + 4.166664568298827e-2) * z * z
    cosine = cosine - 0.5 * z + 1.0
    quarter = turn - 4.0 * jnp.floor(turn * 0.25)
    odd = (quarter == 1.0) | (quarter == 3.0)
    c = jnp.where(odd, sine, cosine)
    s = jnp.where(odd, cosine, sine)
    c = jnp.where((quarter == 1.0) | (quarter == 2.0), -c, c)
    s = jnp.where(quarter >= 2.0, -s, s)
    return c, s


def to_columns(row, count):
    return jnp.transpose(jnp.broadcast_to(row, (lanes, lanes)))[0:count]


def route_block(routes, weight, top_k, expert_count, wide, count):
    tiles = []
    for at in range(0, wide, lanes):
        place = at + lax.broadcasted_iota(jnp.int32, (lanes, lanes), 0)
        lower = place >= expert_count
        expert = jnp.where(lower, place - expert_count, place)
        named = jnp.zeros((lanes, lanes), f32)
        for k in range(top_k):
            named = named + jnp.where(expert == routes[k : k + 1], weight[k : k + 1], 0.0)
        upper = named.astype(bf16).astype(f32)
        kept = jnp.where(lower, named - upper, upper)
        tiles.append(jnp.transpose(kept)[0:count].astype(bf16))
    return tiles


def mixer(
    head_count,
    expert_count,
    tokens_ref,
    lengths_ref,
    routes_ref,
    scores_ref,
    mix_ref,
    ffn_ref,
    wq_hbm,
    wk_hbm,
    wv_hbm,
    wo_hbm,
    keys_hbm,
    values_hbm,
    state_hbm,
    residual_ref,
    block_ref,
    new_keys_ref,
    new_values_ref,
    wq,
    wk,
    wv,
    wo,
    keys,
    values,
    state,
    weights,
    headed,
    small,
    w_sem,
    k_sem,
    v_sem,
    s_sem,
):
    seq_count, block_size, key_width = keys.shape
    key_size = key_width // head_count
    width = tokens_ref.shape[1]
    value_width = values.shape[2]
    value_size = value_width // head_count
    pairs = seq_count // 2

    def load(source, target, sem):
        copy = pltpu.make_async_copy(source, target, sem)
        copy.start()
        return copy

    get_q = load(wq_hbm, wq, w_sem.at[0])
    get_k = load(wk_hbm, wk, w_sem.at[1])
    get_keys = [
        load(keys_hbm.at[pl.ds(2 * p, 2)], keys.at[pl.ds(2 * p, 2)], k_sem.at[p])
        for p in range(pairs)
    ]
    get_v = load(wv_hbm, wv, w_sem.at[2])
    get_values, get_state = [], []
    for p in range(pairs):
        part = pl.ds(2 * p, 2)
        get_values.append(load(values_hbm.at[part], values.at[part], v_sem.at[p]))
        get_state.append(load(state_hbm.at[part], state.at[part], s_sem.at[p]))
    get_o = load(wo_hbm, wo, w_sem.at[3])

    widened = tokens_ref[...].astype(f32)
    normal_in = (widened * inverse_rms(widened) * mix_ref[...]).astype(bf16)

    top_k = routes_ref.shape[0]
    small[...] = jnp.zeros_like(small)
    small[0, 0:1, 0:seq_count] = lengths_ref[...].astype(f32)
    small[1, 0:top_k, 0:seq_count] = routes_ref[...].astype(f32)
    scores = scores_ref[...]
    small[2, 0:top_k, 0:seq_count] = (
        scores / jnp.sum(scores, axis=0, keepdims=True) * route_scale
    )
    positions = to_columns(small[0, 0:1], seq_count)
    lane = lax.broadcasted_iota(jnp.int32, (seq_count, lanes), 1)
    row = lax.broadcasted_iota(jnp.int32, (seq_count, lanes), 0)
    half = key_size // 2
    entry = jnp.where(lane < half, lane, lane - half).astype(f32)
    inverse = jnp.exp(entry * (-math.log(rope_base) / half))
    cosine, sine = cos_sin(positions * inverse)
    signed = jnp.where(lane < half, -sine, sine)
    filled = positions - block_size * jnp.floor(positions * (1.0 / block_size))
    distance = filled - lane.astype(f32)
    live = distance > 0.0
    rates = [math.log1p(-(2.0 ** (-5 - h))) for h in range(head_count)]
    decay = [
        jnp.where(live, jnp.exp(jnp.maximum(distance, 0.0) * rate), 0.0) for rate in rates
    ]

    def rotated(raw):
        return raw * cosine + pltpu.roll(raw, half, 1) * signed

    tiles = route_block(
        small[1].astype(jnp.int32),
        small[2],
        top_k,
        expert_count,
        block_ref.shape[1] - width,
        seq_count,
    )
    for at, tile in enumerate(tiles):
        block_ref[:, width + at * lanes : width + (at + 1) * lanes] = tile

    get_q.wait()
    raw_query = mm(normal_in, wq[...])
    get_k.wait()
    raw_key = mm(normal_in, wk[...])
    queries, own = [], []
    for h in range(head_count):
        part = slice(h * key_size, (h + 1) * key_size)
        query = (rotated(raw_query[:, part]) * key_size ** (-0.5)).astype(bf16)
        key = rotated(raw_key[:, part]).astype(bf16)
        new_keys_ref[:, part] = key
        queries.append(query)
        weight = jnp.sum(query.astype(f32) * key.astype(f32), axis=1, keepdims=True)
        own.append(weight.astype(bf16).astype(f32))

    rows = 2 * block_size
    for p in range(pairs):
        get_keys[p].wait()
        for h in range(head_count):
            stored = keys[2 * p : 2 * p + 2, :, h * key_size : (h + 1) * key_size]
            scores = mm_t(queries[h], stored.reshape(rows, key_size))
            for i in range(2):
                part = scores[:, i * block_size : (i + 1) * block_size] * decay[h]
                weights[h, :, p * rows + i * block_size : p * rows + (i + 1) * block_size] = (
                    jnp.where(row == 2 * p + i, part, 0.0).astype(bf16)
                )

    get_v.wait()
    new_values = mm(normal_in, wv[...]).astype(bf16)
    new_values_ref[...] = new_values

    inside = [jnp.zeros((seq_count, value_size), f32) for _ in range(head_count)]
    carried = [jnp.zeros((seq_count, value_size), f32) for _ in range(head_count)]
    zero = jnp.zeros((seq_count, key_size), bf16)
    for p in range(pairs):
        get_values[p].wait()
        for h in range(head_count):
            stored = values[2 * p : 2 * p + 2, :, h * value_size : (h + 1) * value_size]
            inside[h] = inside[h] + mm(
                weights[h, :, p * rows : (p + 1) * rows], stored.reshape(rows, value_size)
            )
        get_state[p].wait()
        for h in range(head_count):
            chosen = jnp.concatenate(
                [jnp.where(row == 2 * p + i, queries[h].astype(f32), 0.0) for i in range(2)],
                axis=1,
            ).astype(bf16)
            held = state[2 * p : 2 * p + 2, h].reshape(2 * key_size, value_size)
            carried[h] = carried[h] + mm(chosen, held.astype(bf16))

    for h in range(head_count):
        part = slice(h * value_size, (h + 1) * value_size)
        fade = jnp.exp((filled[:, 0:1] + 1.0) * rates[h])
        retained = inside[h] + own[h] * new_values[:, part].astype(f32) + carried[h] * fade
        headed[:, part] = (retained * inverse_rms(retained)).astype(bf16)
    get_o.wait()
    mixer_out = mm(headed[...], wo[...])
    residual = widened + mixer_out * inverse_rms(mixer_out)
    residual_ref[...] = residual
    block_ref[:, 0:width] = (residual * inverse_rms(residual) * ffn_ref[...]).astype(bf16)


def mixed_sequences(
    tokens,
    lengths,
    routes,
    route_scores,
    mix_gain,
    ffn_gain,
    matrices,
    cache_keys,
    cache_values,
    retention_state,
    expert_count,
):
    seq_count, width = tokens.shape
    head_count = retention_state.shape[1]
    extra = 2 * expert_count
    extra += -extra % lanes
    held = [pltpu.VMEM(w.shape, w.dtype) for w in matrices]
    held += [pltpu.VMEM(w.shape, w.dtype) for w in (cache_keys, cache_values, retention_state)]
    dma = pltpu.SemaphoreType.DMA
    vmem = pl.BlockSpec(memory_space=pltpu.VMEM)
    anywhere = pl.BlockSpec(memory_space=pl.ANY)
    return pl.pallas_call(
        functools.partial(mixer, head_count, expert_count),
        out_shape=[
            jax.ShapeDtypeStruct((seq_count, width), f32),
            jax.ShapeDtypeStruct((seq_count, width + extra), bf16),
            jax.ShapeDtypeStruct((seq_count, cache_keys.shape[2]), bf16),
            jax.ShapeDtypeStruct((seq_count, cache_values.shape[2]), bf16),
        ],
        in_specs=[vmem] * 6 + [anywhere] * 7,
        out_specs=[vmem] * 4,
        scratch_shapes=held
        + [
            pltpu.VMEM((head_count, seq_count, seq_count * cache_keys.shape[1]), bf16),
            pltpu.VMEM((seq_count, cache_values.shape[2]), bf16),
            pltpu.VMEM((3, 8, lanes), f32),
            dma((4,)),
            dma((seq_count // 2,)),
            dma((seq_count // 2,)),
            dma((seq_count // 2,)),
        ],
        compiler_params=pltpu.CompilerParams(vmem_limit_bytes=56 * 1024 * 1024),
    )(
        tokens,
        lengths.reshape(1, seq_count),
        routes.T,
        route_scores.T,
        mix_gain.reshape(1, width),
        ffn_gain.reshape(1, width),
        *matrices,
        cache_keys,
        cache_values,
        retention_state,
    )


def slice_dims(device_count):
    side = max(1, math.isqrt(device_count // 8))
    return device_count // (2 * side * side), side, side


def silu(v):
    return v / (1.0 + jnp.exp(-v))


def channel_mixer(
    dims,
    width,
    expert_count,
    block_ref,
    residual_ref,
    mix_ref,
    eg_hbm,
    eu_hbm,
    ed_hbm,
    dg_hbm,
    du_hbm,
    dd_hbm,
    sg_hbm,
    su_hbm,
    sd_hbm,
    out_ref,
    eg,
    eu,
    ed,
    dg,
    du,
    dd,
    sg,
    su,
    sd,
    gathered,
    partial,
    in_core,
    sum_core,
    in2a,
    in2b,
    sum2a,
    sum2b,
    in3a,
    in3b,
    sum3,
    in4,
    total,
    w_sem,
    own_sem,
    gz_s,
    gz_r,
    g2a_s,
    g2a_r,
    g2b_s,
    g2b_r,
    g3a_s,
    g3a_r,
    g3b_s,
    g3b_r,
    g4_s,
    g4_r,
    r1_s,
    r1_r,
    r2a_s,
    r2a_r,
    r2b_s,
    r2b_r,
    r3a_s,
    r3a_r,
    r3b_s,
    r3b_r,
    r4_s,
    r4_r,
):
    zs, ys, xs = dims
    half = width // 2
    me = lax.axis_index("ep")
    core = lax.rem(me, 2)
    x = lax.rem(me // 2, xs)
    y = lax.rem(me // (2 * xs), ys)
    z = me // (2 * xs * ys)
    other = 1 - core

    def turn(at, by, size):
        return lax.rem(at + by + size, size)

    def device(zz, yy, xx, cc):
        return ((zz * ys + yy) * xs + xx) * 2 + cc

    def z_peer(by):
        return device(turn(z, by, zs), y, x, core)

    def y_peer(by):
        return device(z, turn(y, by, ys), x, core)

    def x_peer(by):
        return device(z, y, turn(x, by, xs), core)

    mate = device(z, y, x, other)
    peers = (
        [z_peer(p) for p in range(1, zs)]
        + [y_peer(p) for p in range(1, ys)]
        + [x_peer(p) for p in range(1, xs)]
        + [mate]
    )

    loads = []
    for at, (a, b) in enumerate(
        [
            (sg_hbm, sg),
            (su_hbm, su),
            (sd_hbm, sd),
            (eg_hbm.at[0], eg),
            (eu_hbm.at[0], eu),
            (ed_hbm.at[0], ed),
            (dg_hbm, dg),
            (du_hbm, du),
            (dd_hbm, dd),
        ]
    ):
        load = pltpu.make_async_copy(a, b, w_sem.at[at])
        load.start()
        loads.append(load)
    own = pltpu.make_async_copy(block_ref, gathered.at[z, y, x, core], own_sem)
    own.start()

    barrier = pltpu.get_barrier_semaphore()
    for peer in peers:
        pl.semaphore_signal(
            barrier, inc=1, device_id=(peer,), device_id_type=pl.DeviceIdType.MESH
        )
    pl.semaphore_wait(barrier, len(peers))

    started = []

    def send(source, target, send_sem, recv_sem, peer):
        copy = pltpu.make_async_remote_copy(
            src_ref=source,
            dst_ref=target,
            send_sem=send_sem,
            recv_sem=recv_sem,
            device_id=(peer,),
            device_id_type=pl.DeviceIdType.MESH,
        )
        copy.start()
        started.append(copy)
        return copy

    own.wait()
    for_z, for2, for3, for4 = {}, {}, {}, {}
    for o in range(1, zs):
        mine = gathered.at[z, y, x, core]
        for_z[o] = send(mine, mine, gz_s.at[o - 1], gz_r.at[o - 1], z_peer(o))

    def spread2(o):
        at = turn(z, -o, zs)
        if o:
            for_z[o].wait_recv()
        a = gathered.at[at, y, x, core, :, pl.ds(0, half)]
        b = gathered.at[at, y, x, core, :, pl.ds(half, gathered.shape[-1] - half)]
        for2[o] = [
            send(a, a, g2a_s.at[o, p - 1], g2a_r.at[o, p - 1], y_peer(p)) for p in range(1, ys)
        ] + [send(b, b, g2b_s.at[o, p - 1], g2b_r.at[o, p - 1], x_peer(p)) for p in range(1, xs)]

    def spread3(o):
        at = turn(z, -o, zs)
        for copy in for2[o]:
            copy.wait_recv()
        a = gathered.at[at, :, x, core, :, pl.ds(0, half)]
        b = gathered.at[at, y, :, core, :, pl.ds(half, gathered.shape[-1] - half)]
        for3[o] = [
            send(a, a, g3a_s.at[o, p - 1], g3a_r.at[o, p - 1], x_peer(p)) for p in range(1, xs)
        ] + [send(b, b, g3b_s.at[o, p - 1], g3b_r.at[o, p - 1], y_peer(p)) for p in range(1, ys)]

    def spread4(o):
        at = turn(z, -o, zs)
        for copy in for3[o]:
            copy.wait_recv()
        a = gathered.at[at, :, :, core]
        for4[o] = send(a, a, g4_s.at[o], g4_r.at[o], mate)

    to1, to2, to3, to4 = {}, {}, {}, {}
    gate = 1.0 / (1.0 + jnp.exp(-mix_ref[...]))

    def branches(o):
        at = turn(z, -o, zs)
        if o == 0:
            for load in loads[3:]:
                load.wait()
        for4[o].wait_recv()
        rows = ys * xs * 2 * gathered.shape[4]
        block = gathered[at].reshape(rows, gathered.shape[-1])
        inputs = block[:, :width]
        extra = block[:, width:].astype(f32)
        lane = lax.broadcasted_iota(jnp.int32, extra.shape, 1)
        chosen = (lane == me) | (lane == me + expert_count)
        weight = jnp.sum(jnp.where(chosen, extra, 0.0), axis=1, keepdims=True)
        hidden = (silu(mm(inputs, eg[...])) * mm(inputs, eu[...])).astype(bf16)
        dense = (silu(mm_t(inputs, dg[...])) * mm_t(inputs, du[...])).astype(bf16)
        terms = weight * mm(hidden, ed[...]) + gate * mm(dense, dd[...])
        partial[at] = terms.astype(bf16).reshape(partial.shape[1:])
        to1[o] = send(
            partial.at[at, :, :, other], in_core.at[o], r1_s.at[o], r1_r.at[o], mate
        )

    def reduce2(o):
        at = turn(z, -o, zs)
        to1[o].wait_recv()
        sum_core[o] = (partial[at, :, :, core].astype(f32) + in_core[o].astype(f32)).astype(bf16)
        to2[o] = [
            send(
                sum_core.at[o, :, turn(x, p, xs), :, pl.ds(0, half)],
                in2a.at[o, p - 1],
                r2a_s.at[o, p - 1],
                r2a_r.at[o, p - 1],
                x_peer(p),
            )
            for p in range(1, xs)
        ] + [
            send(
                sum_core.at[o, turn(y, p, ys), :, :, pl.ds(half, width - half)],
                in2b.at[o, p - 1],
                r2b_s.at[o, p - 1],
                r2b_r.at[o, p - 1],
                y_peer(p),
            )
            for p in range(1, ys)
        ]

    def reduce3(o):
        for copy in to2[o]:
            copy.wait_recv()
        a = sum_core[o, :, x, :, 0:half].astype(f32)
        for p in range(1, xs):
            a = a + in2a[o, p - 1].astype(f32)
        sum2a[o] = a.astype(bf16)
        b = sum_core[o, y, :, :, half:width].astype(f32)
        for p in range(1, ys):
            b = b + in2b[o, p - 1].astype(f32)
        sum2b[o] = b.astype(bf16)
        to3[o] = [
            send(
                sum2a.at[o, turn(y, p, ys)],
                in3a.at[o, p - 1],
                r3a_s.at[o, p - 1],
                r3a_r.at[o, p - 1],
                y_peer(p),
            )
            for p in range(1, ys)
        ] + [
            send(
                sum2b.at[o, turn(x, p, xs)],
                in3b.at[o, p - 1],
                r3b_s.at[o, p - 1],
                r3b_r.at[o, p - 1],
                x_peer(p),
            )
            for p in range(1, xs)
        ]

    def reduce4(o):
        for copy in to3[o]:
            copy.wait_recv()
        a = sum2a[o, y].astype(f32)
        for p in range(1, ys):
            a = a + in3a[o, p - 1].astype(f32)
        b = sum2b[o, x].astype(f32)
        for p in range(1, xs):
            b = b + in3b[o, p - 1].astype(f32)
        if o == 0:
            total[:, 0:half] = total[:, 0:half] + a
            total[:, half:width] = total[:, half:width] + b
        else:
            sum3[o - 1, :, 0:half] = a.astype(bf16)
            sum3[o - 1, :, half:width] = b.astype(bf16)
            to4[o] = send(
                sum3.at[o - 1], in4.at[o - 1], r4_s.at[o - 1], r4_r.at[o - 1], z_peer(-o)
            )

    def shared():
        for load in loads[:3]:
            load.wait()
        inputs = block_ref[:, :width]
        hidden = (silu(mm(inputs, sg[...])) * mm(inputs, su[...])).astype(bf16)
        total[...] = mm(hidden, sd[...])

    stages = [spread2, spread3, spread4, branches, reduce2, reduce3, reduce4]
    for step in range(zs + len(stages) - 1):
        for at, stage in enumerate(stages):
            if 0 <= step - at < zs:
                stage(step - at)
        if step == 0:
            shared()

    combined = total[...]
    for o in range(1, zs):
        to4[o].wait_recv()
        combined = combined + in4[o - 1].astype(f32)
    scale = lax.rsqrt(jnp.mean(combined * combined, axis=-1, keepdims=True) + eps)
    out_ref[...] = (residual_ref[...] + combined * scale).astype(bf16)
    for copy in started:
        copy.wait_send()


def mixed_channels(block, residual, dense_mix, weights, expert_count, device_count):
    seq_count, width = residual.shape
    wide = block.shape[1]
    zs, ys, xs = slice_dims(device_count)
    half = width // 2
    rest = width - half
    y1, x1, z1 = max(ys - 1, 1), max(xs - 1, 1), max(zs - 1, 1)
    held = [pltpu.VMEM(w.shape[-2:], bf16) for w in weights]
    dma = pltpu.SemaphoreType.DMA
    buffers = [
        pltpu.VMEM((zs, ys, xs, 2, seq_count, wide), bf16),
        pltpu.VMEM((zs, ys, xs, 2, seq_count, width), bf16),
        pltpu.VMEM((zs, ys, xs, seq_count, width), bf16),
        pltpu.VMEM((zs, ys, xs, seq_count, width), bf16),
        pltpu.VMEM((zs, x1, ys, seq_count, half), bf16),
        pltpu.VMEM((zs, y1, xs, seq_count, rest), bf16),
        pltpu.VMEM((zs, ys, seq_count, half), bf16),
        pltpu.VMEM((zs, xs, seq_count, rest), bf16),
        pltpu.VMEM((zs, y1, seq_count, half), bf16),
        pltpu.VMEM((zs, x1, seq_count, rest), bf16),
        pltpu.VMEM((z1, seq_count, width), bf16),
        pltpu.VMEM((z1, seq_count, width), bf16),
        pltpu.VMEM((seq_count, width), f32),
    ]
    sems = [dma((len(weights),)), dma]
    for shape in [
        (z1,),
        (zs, y1),
        (zs, x1),
        (zs, x1),
        (zs, y1),
        (zs,),
        (zs,),
        (zs, x1),
        (zs, y1),
        (zs, y1),
        (zs, x1),
        (z1,),
    ]:
        sems += [dma(shape), dma(shape)]
    vmem = pl.BlockSpec(memory_space=pltpu.VMEM)
    return pl.pallas_call(
        functools.partial(channel_mixer, (zs, ys, xs), width, expert_count),
        out_shape=jax.ShapeDtypeStruct((seq_count, width), bf16),
        in_specs=[vmem] * 3 + [pl.BlockSpec(memory_space=pl.ANY)] * len(weights),
        out_specs=vmem,
        scratch_shapes=held + buffers + sems,
        compiler_params=pltpu.CompilerParams(
            collective_id=0, has_side_effects=True, vmem_limit_bytes=56 * 1024 * 1024
        ),
    )(block, residual, dense_mix.reshape(1, width), *weights)


def per_device(
    tokens,
    lengths,
    cache_keys,
    cache_values,
    retention_state,
    mix_gain,
    query_weight,
    key_weight,
    value_weight,
    out_weight,
    ffn_gain,
    routes,
    route_scores,
    expert_gate,
    expert_up,
    expert_down,
    shared_gate,
    shared_up,
    shared_down,
    dense_gate,
    dense_up,
    dense_down,
    dense_mix,
):
    device_count = lax.axis_size("ep")
    expert_count = device_count * expert_gate.shape[0]
    residual, block, new_keys, new_values = mixed_sequences(
        tokens,
        lengths,
        routes,
        route_scores,
        mix_gain,
        ffn_gain,
        (query_weight, key_weight, value_weight, out_weight),
        cache_keys,
        cache_values,
        retention_state,
        expert_count,
    )
    weights = (
        expert_gate,
        expert_up,
        expert_down,
        dense_gate,
        dense_up,
        dense_down,
        shared_gate,
        shared_up,
        shared_down,
    )
    layer_out = mixed_channels(block, residual, dense_mix, weights, expert_count, device_count)
    return (layer_out, new_keys, new_values)


def solution(mesh):
    in_specs = (
        P("ep", None),
        P("ep"),
        P("ep", None, None),
        P("ep", None, None),
        P("ep", None, None, None),
        P(),
        P(),
        P(),
        P(),
        P(),
        P(),
        P("ep", None),
        P("ep", None),
        P("ep", None, None),
        P("ep", None, None),
        P("ep", None, None),
        P(),
        P(),
        P(),
        P("ep", None),
        P("ep", None),
        P("ep", None),
        P(),
    )
    out_specs = (P("ep", None), P("ep", None), P("ep", None))
    return jax.shard_map(
        per_device, mesh=mesh, in_specs=in_specs, out_specs=out_specs, check_vma=False
    )
```

```python
import functools
import math

import jax
import jax.numpy as jnp
from jax import lax
from jax.experimental import pallas as pl
from jax.experimental.pallas import tpu as pltpu
from jax.sharding import PartitionSpec as P

eps = 1e-06
route_scale = 2.5
rope_base = 10000.0

f32 = jnp.float32
bf16 = jnp.bfloat16
lanes = 128


def inverse_rms(values):
    return lax.rsqrt(jnp.mean(values * values, axis=-1, keepdims=True) + eps)


def mm(a, b):
    return lax.dot_general(a, b, (((1,), (0,)), ((), ())), preferred_element_type=f32)


def mm_t(a, b):
    return lax.dot_general(a, b, (((1,), (1,)), ((), ())), preferred_element_type=f32)


def cos_sin(angles):
    turn = jnp.floor(angles * (2.0 / math.pi) + 0.5)
    r = angles - turn * 1.5703125
    r = r - turn * 4.837512969970703125e-4
    r = r - turn * 7.54978995489188216e-8
    z = r * r
    sine = ((-1.9515295891e-4 * z + 8.3321608736e-3) * z - 1.6666654611e-1) * z * r + r
    cosine = ((2.443315711809948e-5 * z - 1.388731625493765e-3) * z + 4.166664568298827e-2) * z * z
    cosine = cosine - 0.5 * z + 1.0
    quarter = turn - 4.0 * jnp.floor(turn * 0.25)
    odd = (quarter == 1.0) | (quarter == 3.0)
    c = jnp.where(odd, sine, cosine)
    s = jnp.where(odd, cosine, sine)
    c = jnp.where((quarter == 1.0) | (quarter == 2.0), -c, c)
    s = jnp.where(quarter >= 2.0, -s, s)
    return c, s


def to_columns(row, count):
    return jnp.transpose(jnp.broadcast_to(row, (lanes, lanes)))[0:count]


def route_block(routes, weight, top_k, expert_count, wide, count):
    tiles = []
    for at in range(0, wide, lanes):
        place = at + lax.broadcasted_iota(jnp.int32, (lanes, lanes), 0)
        lower = place >= expert_count
        expert = jnp.where(lower, place - expert_count, place)
        named = jnp.zeros((lanes, lanes), f32)
        for k in range(top_k):
            named = named + jnp.where(expert == routes[k : k + 1], weight[k : k + 1], 0.0)
        upper = named.astype(bf16).astype(f32)
        kept = jnp.where(lower, named - upper, upper)
        tiles.append(jnp.transpose(kept)[0:count].astype(bf16))
    return tiles


def silu(v):
    return v / (1.0 + jnp.exp(-v))


def slice_dims(device_count):
    side = max(1, math.isqrt(device_count // 8))
    return device_count // (2 * side * side), side, side


def crossed(at, by):
    moved, bit = at, 1
    while bit <= by:
        if by & bit:
            moved = moved + bit - 2 * bit * lax.rem(at // bit, 2)
        bit *= 2
    return moved


def layer(
    dims,
    head_count,
    expert_count,
    tokens_ref,
    lengths_ref,
    routes_ref,
    scores_ref,
    mix_ref,
    ffn_ref,
    dense_ref,
    wq_hbm,
    wk_hbm,
    wv_hbm,
    wo_hbm,
    keys_hbm,
    values_hbm,
    state_hbm,
    eg_hbm,
    eu_hbm,
    ed_hbm,
    dg_hbm,
    du_hbm,
    dd_hbm,
    sg_hbm,
    su_hbm,
    sd_hbm,
    out_ref,
    new_keys_ref,
    new_values_ref,
    wq,
    wk,
    wv,
    wo,
    keys,
    values,
    state,
    eg,
    eu,
    ed,
    dg,
    du,
    dd,
    sg,
    su,
    sd,
    weights,
    headed,
    small,
    extras,
    gathered,
    partial,
    arrived,
    summed,
    returned,
    w_sem,
    k_sem,
    v_sem,
    s_sem,
    f_sem,
    swap_s,
    swap_r,
    ez_s,
    ez_r,
    ep_s,
    ep_r,
    z_s,
    z_r,
    d_s,
    d_r,
    p_s,
    p_r,
    b_s,
    b_r,
):
    seq_count, block_size, key_width = keys.shape
    key_size = key_width // head_count
    width = tokens_ref.shape[1]
    value_width = values.shape[2]
    value_size = value_width // head_count
    pairs = seq_count // 2

    zs, ys, xs = dims
    me = lax.axis_index("ep")
    core = lax.rem(me, 2)
    x = lax.rem(me // 2, xs)
    y = lax.rem(me // (2 * xs), ys)
    z = me // (2 * xs * ys)
    paired = zs & (zs - 1) == 0

    def device(zz, yy, xx, cc):
        return ((zz * ys + yy) * xs + xx) * 2 + cc

    def source(o):
        return crossed(z, o) if paired else lax.rem(z - o + zs, zs)

    def target(o):
        return crossed(z, o) if paired else lax.rem(z + o, zs)

    around = [(dy, dx) for dy in range(ys) for dx in range(xs) if dy or dx]

    def beside(i):
        dy, dx = around[i]
        return lax.rem(y + dy, ys), lax.rem(x + dx, xs)

    mate = device(z, y, x, 1 - core)
    z_peers = [device(target(o), y, x, core) for o in range(1, zs)]
    home_peers = [device(source(o), y, x, core) for o in range(1, zs)]
    plane_peers = [device(z, *beside(i), core) for i in range(len(around))]

    def load(origin, place, sem):
        copy = pltpu.make_async_copy(origin, place, sem)
        copy.start()
        return copy

    get_q = load(wq_hbm, wq, w_sem.at[0])
    get_k = load(wk_hbm, wk, w_sem.at[1])
    get_keys = [
        load(keys_hbm.at[pl.ds(2 * p, 2)], keys.at[pl.ds(2 * p, 2)], k_sem.at[p])
        for p in range(pairs)
    ]
    get_ffn = [
        load(origin, place, f_sem.at[at])
        for at, (origin, place) in enumerate(
            [
                (eg_hbm, eg.at[pl.ds(0, 1)]),
                (eu_hbm, eu.at[pl.ds(0, 1)]),
                (ed_hbm, ed.at[pl.ds(0, 1)]),
                (dg_hbm, dg.at[0]),
                (du_hbm, du.at[0]),
                (dd_hbm, dd.at[0]),
            ]
        )
    ]
    get_v = load(wv_hbm, wv, w_sem.at[2])
    get_values, get_state = [], []
    for p in range(pairs):
        part = pl.ds(2 * p, 2)
        get_values.append(load(values_hbm.at[part], values.at[part], v_sem.at[p]))
        get_state.append(load(state_hbm.at[part], state.at[part], s_sem.at[p]))
    get_o = load(wo_hbm, wo, w_sem.at[3])
    get_shared = [
        load(origin, place, f_sem.at[6 + at])
        for at, (origin, place) in enumerate([(sg_hbm, sg), (su_hbm, su), (sd_hbm, sd)])
    ]

    barrier = pltpu.get_barrier_semaphore()
    peers = z_peers + plane_peers + [mate]
    if not paired:
        peers = peers + home_peers
    for peer in peers:
        pl.semaphore_signal(
            barrier, inc=1, device_id=(peer,), device_id_type=pl.DeviceIdType.MESH
        )

    started = []

    def send(origin, place, send_sem, recv_sem, peer):
        copy = pltpu.make_async_remote_copy(
            src_ref=origin,
            dst_ref=place,
            send_sem=send_sem,
            recv_sem=recv_sem,
            device_id=(peer,),
            device_id_type=pl.DeviceIdType.MESH,
        )
        copy.start()
        started.append(copy)
        return copy

    widened = tokens_ref[...].astype(f32)
    normal_in = (widened * inverse_rms(widened) * mix_ref[...]).astype(bf16)

    top_k = routes_ref.shape[0]
    small[...] = jnp.zeros_like(small)
    small[0, 0:1, 0:seq_count] = lengths_ref[...].astype(f32)
    small[1, 0:top_k, 0:seq_count] = routes_ref[...].astype(f32)
    scores = scores_ref[...]
    small[2, 0:top_k, 0:seq_count] = (
        scores / jnp.sum(scores, axis=0, keepdims=True) * route_scale
    )
    tiles = route_block(
        small[1].astype(jnp.int32),
        small[2],
        top_k,
        expert_count,
        extras.shape[-1],
        seq_count,
    )
    for at, tile in enumerate(tiles):
        extras[z, y, x, :, at * lanes : (at + 1) * lanes] = tile

    positions = to_columns(small[0, 0:1], seq_count)
    lane = lax.broadcasted_iota(jnp.int32, (seq_count, lanes), 1)
    row = lax.broadcasted_iota(jnp.int32, (seq_count, lanes), 0)
    half = key_size // 2
    entry = jnp.where(lane < half, lane, lane - half).astype(f32)
    inverse = jnp.exp(entry * (-math.log(rope_base) / half))
    cosine, sine = cos_sin(positions * inverse)
    signed = jnp.where(lane < half, -sine, sine)
    filled = positions - block_size * jnp.floor(positions * (1.0 / block_size))
    distance = filled - lane.astype(f32)
    live = distance > 0.0
    rates = [math.log1p(-(2.0 ** (-5 - h))) for h in range(head_count)]
    decay = [
        jnp.where(live, jnp.exp(jnp.maximum(distance, 0.0) * rate), 0.0) for rate in rates
    ]

    def rotated(raw):
        return raw * cosine + pltpu.roll(raw, half, 1) * signed

    get_q.wait()
    raw_query = mm(normal_in, wq[...])
    get_k.wait()
    raw_key = mm(normal_in, wk[...])
    queries, own = [], []
    for h in range(head_count):
        part = slice(h * key_size, (h + 1) * key_size)
        query = (rotated(raw_query[:, part]) * key_size ** (-0.5)).astype(bf16)
        key = rotated(raw_key[:, part]).astype(bf16)
        new_keys_ref[:, part] = key
        queries.append(query)
        weight = jnp.sum(query.astype(f32) * key.astype(f32), axis=1, keepdims=True)
        own.append(weight.astype(bf16).astype(f32))

    pl.semaphore_wait(barrier, len(peers))
    mine = extras.at[z, y, x]
    extra_z = [
        send(mine, mine, ez_s.at[o - 1], ez_r.at[o - 1], z_peers[o - 1]) for o in range(1, zs)
    ]

    rows = 2 * block_size
    for p in range(pairs):
        get_keys[p].wait()
        for h in range(head_count):
            stored = keys[2 * p : 2 * p + 2, :, h * key_size : (h + 1) * key_size]
            scores = mm_t(queries[h], stored.reshape(rows, key_size))
            for i in range(2):
                part = scores[:, i * block_size : (i + 1) * block_size] * decay[h]
                weights[h, :, p * rows + i * block_size : p * rows + (i + 1) * block_size] = (
                    jnp.where(row == 2 * p + i, part, 0.0).astype(bf16)
                )

    swaps = []
    for at, (copy, held) in enumerate(zip(get_ffn, (eg, eu, ed, dg, du, dd))):
        copy.wait()
        swaps.append(send(held.at[0], held.at[1], swap_s.at[at], swap_r.at[at], mate))
    for copy in extra_z:
        copy.wait_recv()
    column = extras.at[:, y, x]
    extra_plane = [
        send(column, column, ep_s.at[i], ep_r.at[i], plane_peers[i]) for i in range(len(around))
    ]

    get_v.wait()
    new_values = mm(normal_in, wv[...]).astype(bf16)
    new_values_ref[...] = new_values

    inside = [jnp.zeros((seq_count, value_size), f32) for _ in range(head_count)]
    carried = [jnp.zeros((seq_count, value_size), f32) for _ in range(head_count)]
    for p in range(pairs):
        get_values[p].wait()
        for h in range(head_count):
            stored = values[2 * p : 2 * p + 2, :, h * value_size : (h + 1) * value_size]
            inside[h] = inside[h] + mm(
                weights[h, :, p * rows : (p + 1) * rows], stored.reshape(rows, value_size)
            )
        get_state[p].wait()
        for h in range(head_count):
            chosen = jnp.concatenate(
                [jnp.where(row == 2 * p + i, queries[h].astype(f32), 0.0) for i in range(2)],
                axis=1,
            ).astype(bf16)
            held = state[2 * p : 2 * p + 2, h].reshape(2 * key_size, value_size)
            carried[h] = carried[h] + mm(chosen, held.astype(bf16))

    for h in range(head_count):
        part = slice(h * value_size, (h + 1) * value_size)
        fade = jnp.exp((filled[:, 0:1] + 1.0) * rates[h])
        retained = inside[h] + own[h] * new_values[:, part].astype(f32) + carried[h] * fade
        headed[:, part] = (retained * inverse_rms(retained)).astype(bf16)
    get_o.wait()
    mixer_out = mm(headed[...], wo[...])
    residual = widened + mixer_out * inverse_rms(mixer_out)
    normal_ffn = (residual * inverse_rms(residual) * ffn_ref[...]).astype(bf16)
    gathered[z, y, x] = normal_ffn

    block = gathered.at[z, y, x]
    from_z = [None] + [
        send(block, block, z_s.at[o - 1], z_r.at[o - 1], z_peers[o - 1]) for o in range(1, zs)
    ]

    def spread(o):
        if o:
            from_z[o].wait_recv()
        part = gathered.at[source(o), y, x]
        return [
            send(part, part, d_s.at[o, i], d_r.at[o, i], plane_peers[i])
            for i in range(len(around))
        ]

    from_plane = [spread(0)]

    for copy in get_shared:
        copy.wait()
    hidden = (silu(mm(normal_ffn, sg[...])) * mm(normal_ffn, su[...])).astype(bf16)
    combined = mm(hidden, sd[...])
    gate = 1.0 / (1.0 + jnp.exp(-dense_ref[...]))

    for o in range(1, zs):
        from_plane.append(spread(o))
    for copy in swaps + extra_plane:
        copy.wait_recv()

    def branches(o):
        at = source(o)
        for copy in from_plane[o]:
            copy.wait_recv()
        count = ys * xs * seq_count
        inputs = gathered[at].reshape(count, width)
        scale = extras[at].reshape(count, extras.shape[-1]).astype(f32)
        place = lax.broadcasted_iota(jnp.int32, scale.shape, 1)
        dense = (
            silu(mm_t(inputs, dg[...].reshape(-1, width)))
            * mm_t(inputs, du[...].reshape(-1, width))
        ).astype(bf16)
        terms = gate * mm(dense, dd[...].reshape(-1, width))
        for slot, expert in enumerate((me, mate)):
            chosen = (place == expert) | (place == expert + expert_count)
            weight = jnp.sum(jnp.where(chosen, scale, 0.0), axis=1, keepdims=True)
            inner = (silu(mm(inputs, eg[slot])) * mm(inputs, eu[slot])).astype(bf16)
            terms = terms + weight * mm(inner, ed[slot])
        partial[at] = terms.astype(bf16).reshape(partial.shape[1:])
        return [
            send(
                partial.at[at, beside(i)[0], beside(i)[1]],
                arrived.at[o, i],
                p_s.at[o, i],
                p_r.at[o, i],
                plane_peers[i],
            )
            for i in range(len(around))
        ]

    to_plane = [branches(o) for o in range(zs)]

    def plane_sum(o):
        for copy in to_plane[o]:
            copy.wait_recv()
        value = partial[source(o), y, x].astype(f32)
        for i in range(len(around)):
            value = value + arrived[o, i].astype(f32)
        return value

    combined = combined + plane_sum(0)
    to_home = []
    for o in range(1, zs):
        summed[o - 1] = plane_sum(o).astype(bf16)
        to_home.append(
            send(
                summed.at[o - 1],
                returned.at[o - 1],
                b_s.at[o - 1],
                b_r.at[o - 1],
                home_peers[o - 1],
            )
        )
    for o in range(1, zs):
        to_home[o - 1].wait_recv()
        combined = combined + returned[o - 1].astype(f32)
    out_ref[...] = (residual + combined * inverse_rms(combined)).astype(bf16)
    for copy in started:
        copy.wait_send()


def finish(a_ref, b_ref, c_ref, a_out, b_out, c_out, sems):
    copies = [
        pltpu.make_async_copy(origin, place, sems.at[at])
        for at, (origin, place) in enumerate([(a_ref, a_out), (b_ref, b_out), (c_ref, c_out)])
    ]
    for copy in copies:
        copy.start()
    for copy in copies:
        copy.wait()


def whole_layer(vectors, streams, shapes, dims, expert_count):
    seq_count, width, head_count, top_k = shapes
    zs, ys, xs = dims
    wq, wk, wv, wo, keys, values, state = streams[:7]
    experts, dense, shared = streams[7:10], streams[10:13], streams[13:16]
    z1, others = max(zs - 1, 1), max(ys * xs - 1, 1)
    extra = 2 * expert_count
    extra += -extra % lanes
    dma = pltpu.SemaphoreType.DMA
    vmem = pl.BlockSpec(memory_space=pltpu.VMEM)
    anywhere = pl.BlockSpec(memory_space=pl.ANY)
    grid = (zs, ys, xs, seq_count)
    scratch = [pltpu.VMEM(w.shape, w.dtype) for w in streams[:7]]
    scratch += [pltpu.VMEM((2,) + w.shape[1:], bf16) for w in experts]
    scratch += [pltpu.VMEM((2,) + w.shape, bf16) for w in dense]
    scratch += [pltpu.VMEM(w.shape, bf16) for w in shared]
    scratch += [
        pltpu.VMEM((head_count, seq_count, seq_count * keys.shape[1]), bf16),
        pltpu.VMEM((seq_count, values.shape[2]), bf16),
        pltpu.VMEM((3, 8, lanes), f32),
        pltpu.VMEM(grid + (extra,), bf16),
        pltpu.VMEM(grid + (width,), bf16),
        pltpu.VMEM(grid + (width,), bf16),
        pltpu.VMEM((zs, others, seq_count, width), bf16),
        pltpu.VMEM((z1, seq_count, width), bf16),
        pltpu.VMEM((z1, seq_count, width), bf16),
    ]
    pairs = (seq_count // 2,)
    sems = [(4,), pairs, pairs, pairs, (9,), (6,), (6,), (z1,), (z1,), (others,), (others,)]
    sems += [(z1,), (z1,)] + [(zs, others)] * 4 + [(z1,), (z1,)]
    out_shapes = [(seq_count, width), (seq_count, keys.shape[2]), (seq_count, values.shape[2])]
    results = pl.pallas_call(
        functools.partial(layer, dims, head_count, expert_count),
        out_shape=[pltpu.VMEM(shape, bf16) for shape in out_shapes],
        in_specs=[vmem] * len(vectors) + [anywhere] * len(streams),
        out_specs=[vmem] * 3,
        scratch_shapes=scratch + [dma(shape) for shape in sems],
        compiler_params=pltpu.CompilerParams(
            collective_id=0, has_side_effects=True, vmem_limit_bytes=58 * 1024 * 1024
        ),
    )(*vectors, *streams)
    return pl.pallas_call(
        finish,
        out_shape=[jax.ShapeDtypeStruct(shape, bf16) for shape in out_shapes],
        in_specs=[vmem] * 3,
        out_specs=[anywhere] * 3,
        scratch_shapes=[dma((3,))],
        compiler_params=pltpu.CompilerParams(vmem_limit_bytes=1024 * 1024),
    )(*results)


def per_device(
    tokens,
    lengths,
    cache_keys,
    cache_values,
    retention_state,
    mix_gain,
    query_weight,
    key_weight,
    value_weight,
    out_weight,
    ffn_gain,
    routes,
    route_scores,
    expert_gate,
    expert_up,
    expert_down,
    shared_gate,
    shared_up,
    shared_down,
    dense_gate,
    dense_up,
    dense_down,
    dense_mix,
):
    device_count = lax.axis_size("ep")
    expert_count = device_count * expert_gate.shape[0]
    seq_count, width = tokens.shape
    vectors = (
        tokens,
        lengths.reshape(1, seq_count),
        routes.T,
        route_scores.T,
        mix_gain.reshape(1, width),
        ffn_gain.reshape(1, width),
        dense_mix.reshape(1, width),
    )
    streams = (
        query_weight,
        key_weight,
        value_weight,
        out_weight,
        cache_keys,
        cache_values,
        retention_state,
        expert_gate,
        expert_up,
        expert_down,
        dense_gate,
        dense_up,
        dense_down,
        shared_gate,
        shared_up,
        shared_down,
    )
    shapes = (seq_count, width, retention_state.shape[1], routes.shape[1])
    return tuple(
        whole_layer(vectors, streams, shapes, slice_dims(device_count), expert_count)
    )


def solution(mesh):
    in_specs = (
        P("ep", None),
        P("ep"),
        P("ep", None, None),
        P("ep", None, None),
        P("ep", None, None, None),
        P(),
        P(),
        P(),
        P(),
        P(),
        P(),
        P("ep", None),
        P("ep", None),
        P("ep", None, None),
        P("ep", None, None),
        P("ep", None, None),
        P(),
        P(),
        P(),
        P("ep", None),
        P("ep", None),
        P("ep", None),
        P(),
    )
    out_specs = (P("ep", None), P("ep", None), P("ep", None))
    return jax.shard_map(
        per_device, mesh=mesh, in_specs=in_specs, out_specs=out_specs, check_vma=False
    )
```

```python
import functools
import math

import jax
import jax.numpy as jnp
from jax import lax
from jax.experimental import pallas as pl
from jax.experimental.pallas import tpu as pltpu
from jax.sharding import PartitionSpec as P

eps = 1e-06
route_scale = 2.5
rope_base = 10000.0

f32 = jnp.float32
bf16 = jnp.bfloat16
lanes = 128


def inverse_rms(values):
    return lax.rsqrt(jnp.mean(values * values, axis=-1, keepdims=True) + eps)


def mm(a, b):
    return lax.dot_general(a, b, (((1,), (0,)), ((), ())), preferred_element_type=f32)


def mm_t(a, b):
    return lax.dot_general(a, b, (((1,), (1,)), ((), ())), preferred_element_type=f32)


def cos_sin(angles):
    turn = jnp.floor(angles * (2.0 / math.pi) + 0.5)
    r = angles - turn * 1.5703125
    r = r - turn * 4.837512969970703125e-4
    r = r - turn * 7.54978995489188216e-8
    z = r * r
    sine = ((-1.9515295891e-4 * z + 8.3321608736e-3) * z - 1.6666654611e-1) * z * r + r
    cosine = ((2.443315711809948e-5 * z - 1.388731625493765e-3) * z + 4.166664568298827e-2) * z * z
    cosine = cosine - 0.5 * z + 1.0
    quarter = turn - 4.0 * jnp.floor(turn * 0.25)
    odd = (quarter == 1.0) | (quarter == 3.0)
    c = jnp.where(odd, sine, cosine)
    s = jnp.where(odd, cosine, sine)
    c = jnp.where((quarter == 1.0) | (quarter == 2.0), -c, c)
    s = jnp.where(quarter >= 2.0, -s, s)
    return c, s


def to_columns(row, count):
    return jnp.transpose(jnp.broadcast_to(row, (lanes, lanes)))[0:count]


def route_block(routes, weight, top_k, expert_count, wide, count):
    tiles = []
    for at in range(0, wide, lanes):
        place = at + lax.broadcasted_iota(jnp.int32, (lanes, lanes), 0)
        lower = place >= expert_count
        expert = jnp.where(lower, place - expert_count, place)
        named = jnp.zeros((lanes, lanes), f32)
        for k in range(top_k):
            named = named + jnp.where(expert == routes[k : k + 1], weight[k : k + 1], 0.0)
        upper = named.astype(bf16).astype(f32)
        kept = jnp.where(lower, named - upper, upper)
        tiles.append(jnp.transpose(kept)[0:count].astype(bf16))
    return tiles


def silu(v):
    return v / (1.0 + jnp.exp(-v))


def slice_dims(device_count):
    side = max(1, math.isqrt(device_count // 8))
    return device_count // (2 * side * side), side, side


def layer(
    dims,
    head_count,
    expert_count,
    tokens_hbm,
    lengths_hbm,
    routes_hbm,
    scores_hbm,
    mix_hbm,
    ffn_hbm,
    dense_hbm,
    wq_hbm,
    wk_hbm,
    wv_hbm,
    wo_hbm,
    keys_hbm,
    values_hbm,
    state_hbm,
    eg_hbm,
    eu_hbm,
    ed_hbm,
    dg_hbm,
    du_hbm,
    dd_hbm,
    sg_hbm,
    su_hbm,
    sd_hbm,
    out_ref,
    new_keys_ref,
    new_values_ref,
    tokens_ref,
    lengths_ref,
    routes_ref,
    scores_ref,
    mix_ref,
    ffn_ref,
    dense_ref,
    wq,
    wk,
    wv,
    wo,
    keys,
    values,
    state,
    eg,
    eu,
    ed,
    dg,
    du,
    dd,
    sg,
    su,
    sd,
    weights,
    small,
    extras,
    gathered,
    partial,
    arrived,
    summed,
    returned,
    l_sem,
    swap_s,
    swap_r,
    ez_s,
    ez_r,
    ep_s,
    ep_r,
    z_s,
    z_r,
    d_s,
    d_r,
    p_s,
    p_r,
    b_s,
    b_r,
):
    seq_count, block_size, key_width = keys.shape
    key_size = key_width // head_count
    width = tokens_ref.shape[1]
    value_width = values.shape[2]
    value_size = value_width // head_count
    pairs = seq_count // 2

    zs, ys, xs = dims
    me = lax.axis_index("ep")
    core = lax.rem(me, 2)
    x = lax.rem(me // 2, xs)
    y = lax.rem(me // (2 * xs), ys)
    z = me // (2 * xs * ys)

    def device(zz, yy, xx, cc):
        return ((zz * ys + yy) * xs + xx) * 2 + cc

    planes = [k + (k - z + zs) // zs for k in range(zs - 1)]
    around = sorted(
        ((dy, dx) for dy in range(ys) for dx in range(xs) if dy or dx),
        key=lambda step: -min(step[0], ys - step[0]) - min(step[1], xs - step[1]),
    )

    def beside(i):
        dy, dx = around[i]
        return lax.rem(y + dy, ys), lax.rem(x + dx, xs)

    def behind(i):
        dy, dx = around[i]
        return lax.rem(y - dy + ys, ys), lax.rem(x - dx + xs, xs)

    mate = device(z, y, x, 1 - core)
    z_peers = [device(plane, y, x, core) for plane in planes]
    plane_peers = [device(z, *beside(i), core) for i in range(len(around))]

    waiting = []

    def plan(name, origin, place, pieces=1):
        count = origin.shape[0] // pieces
        for at in range(pieces):
            part = pl.ds(at * count, count)
            index = len(waiting)
            copy = pltpu.make_async_copy(origin.at[part], place.at[part], l_sem.at[index])
            waiting.append((name, copy))

    plan("tokens", tokens_hbm, tokens_ref)
    plan("tokens", mix_hbm, mix_ref)
    plan("query", wq_hbm, wq, 2)
    plan("small", lengths_hbm, lengths_ref)
    plan("small", routes_hbm, routes_ref)
    plan("small", scores_hbm, scores_ref)
    plan("key", wk_hbm, wk, 2)
    for p in range(0, pairs, 2):
        part = pl.ds(2 * p, 4)
        plan(("keys", p), keys_hbm.at[part], keys.at[part])
    plan("value", wv_hbm, wv, 4)
    for p in range(pairs):
        part = pl.ds(2 * p, 2)
        plan(("values", p), values_hbm.at[part], values.at[part])
        plan(("state", p), state_hbm.at[part], state.at[part], 2)
        if p == 0:
            plan("swap", eg_hbm, eg.at[pl.ds(0, 1)])
            plan("swap", eu_hbm, eu.at[pl.ds(0, 1)])
            plan("swap", ed_hbm, ed.at[pl.ds(0, 1)])
            plan("swap", dg_hbm, dg.at[0])
            plan("swap", du_hbm, du.at[0])
            plan("swap", dd_hbm, dd.at[0])
        if p == pairs // 2 - 1:
            plan("out", wo_hbm, wo, 4)
            plan("out", ffn_hbm, ffn_ref)
    plan("shared", sg_hbm, sg)
    plan("shared", su_hbm, su)
    plan("shared", sd_hbm, sd)
    plan("shared", dense_hbm, dense_ref)

    for _, copy in waiting:
        copy.start()

    def need(name):
        for label, copy in waiting:
            if label == name:
                copy.wait()

    barrier = pltpu.get_barrier_semaphore()
    peers = z_peers + plane_peers + [mate]
    for peer in peers:
        pl.semaphore_signal(
            barrier, inc=1, device_id=(peer,), device_id_type=pl.DeviceIdType.MESH
        )

    started = []

    def send(origin, place, send_sem, recv_sem, peer):
        copy = pltpu.make_async_remote_copy(
            src_ref=origin,
            dst_ref=place,
            send_sem=send_sem,
            recv_sem=recv_sem,
            device_id=(peer,),
            device_id_type=pl.DeviceIdType.MESH,
        )
        copy.start()
        started.append(copy)

    def landed(place, sem):
        pltpu.make_async_remote_copy(
            src_ref=place,
            dst_ref=place,
            send_sem=sem,
            recv_sem=sem,
            device_id=(mate,),
            device_id_type=pl.DeviceIdType.MESH,
        ).wait_recv()

    need("tokens")
    widened = tokens_ref[...].astype(f32)
    normal_in = (widened * inverse_rms(widened) * mix_ref[...]).astype(bf16)

    need("small")
    top_k = routes_ref.shape[0]
    small[...] = jnp.zeros_like(small)
    small[0, 0:1, 0:seq_count] = lengths_ref[...].astype(f32)
    small[1, 0:top_k, 0:seq_count] = routes_ref[...].astype(f32)
    scores = scores_ref[...]
    small[2, 0:top_k, 0:seq_count] = (
        scores / jnp.sum(scores, axis=0, keepdims=True) * route_scale
    )
    tiles = route_block(
        small[1].astype(jnp.int32),
        small[2],
        top_k,
        expert_count,
        extras.shape[-1],
        seq_count,
    )
    for at, tile in enumerate(tiles):
        extras[z, y, x, :, at * lanes : (at + 1) * lanes] = tile

    positions = to_columns(small[0, 0:1], seq_count)
    lane = lax.broadcasted_iota(jnp.int32, (seq_count, lanes), 1)
    row = lax.broadcasted_iota(jnp.int32, (seq_count, lanes), 0)
    half = key_size // 2
    entry = jnp.where(lane < half, lane, lane - half).astype(f32)
    inverse = jnp.exp(entry * (-math.log(rope_base) / half))
    cosine, sine = cos_sin(positions * inverse)
    signed = jnp.where(lane < half, -sine, sine)
    filled = positions - block_size * jnp.floor(positions * (1.0 / block_size))
    distance = filled - lane.astype(f32)
    live = distance > 0.0
    rates = [math.log1p(-(2.0 ** (-5 - h))) for h in range(head_count)]
    decay = [
        jnp.where(live, jnp.exp(jnp.maximum(distance, 0.0) * rate), 0.0) for rate in rates
    ]

    def rotated(raw):
        return raw * cosine + pltpu.roll(raw, half, 1) * signed

    need("query")
    raw_query = mm(normal_in, wq[...])
    need("key")
    raw_key = mm(normal_in, wk[...])
    queries, own = [], []
    for h in range(head_count):
        part = slice(h * key_size, (h + 1) * key_size)
        query = (rotated(raw_query[:, part]) * key_size ** (-0.5)).astype(bf16)
        key = rotated(raw_key[:, part]).astype(bf16)
        new_keys_ref[:, part] = key
        queries.append(query)
        weight = jnp.sum(query.astype(f32) * key.astype(f32), axis=1, keepdims=True)
        own.append(weight.astype(bf16).astype(f32))

    pl.semaphore_wait(barrier, len(peers))
    mine = extras.at[z, y, x]
    for k, peer in enumerate(z_peers):
        send(mine, mine, ez_s.at[k], ez_r.at[z], peer)

    rows = 2 * block_size
    for p in range(pairs):
        if p % 2 == 0:
            need(("keys", p))
        for h in range(head_count):
            stored = keys[2 * p : 2 * p + 2, :, h * key_size : (h + 1) * key_size]
            scores = mm_t(queries[h], stored.reshape(rows, key_size))
            for i in range(2):
                part = scores[:, i * block_size : (i + 1) * block_size] * decay[h]
                weights[h, :, p * rows + i * block_size : p * rows + (i + 1) * block_size] = (
                    jnp.where(row == 2 * p + i, part, 0.0).astype(bf16)
                )

    need("value")
    new_values = mm(normal_in, wv[...]).astype(bf16)
    new_values_ref[...] = new_values

    wide_values = new_values.astype(f32)
    inside = [jnp.zeros((seq_count, value_size), f32) for _ in range(head_count)]
    carried = [jnp.zeros((seq_count, value_size), f32) for _ in range(head_count)]
    fades = [jnp.exp((filled[:, 0:1] + 1.0) * rate) for rate in rates]
    residuals = []
    part_rows = seq_count // 2

    def piece(at, q):
        return gathered.at[at, y, x, pl.ds(q * part_rows, part_rows)]

    def spread(q, at):
        part = piece(at, q)
        for i, peer in enumerate(plane_peers):
            send(part, part, d_s.at[q, at, i], d_r.at[q, at, i], peer)

    for p in range(pairs):
        need(("values", p))
        for h in range(head_count):
            stored = values[2 * p : 2 * p + 2, :, h * value_size : (h + 1) * value_size]
            inside[h] = inside[h] + mm(
                weights[h, :, p * rows : (p + 1) * rows], stored.reshape(rows, value_size)
            )
        need(("state", p))
        for h in range(head_count):
            chosen = jnp.concatenate(
                [jnp.where(row == 2 * p + i, queries[h].astype(f32), 0.0) for i in range(2)],
                axis=1,
            ).astype(bf16)
            held = state[2 * p : 2 * p + 2, h].reshape(2 * key_size, value_size)
            carried[h] = carried[h] + mm(chosen, held.astype(bf16))
        if p == 1:
            need("swap")
            for at, held in enumerate((eg, eu, ed, dg, du, dd)):
                send(held.at[0], held.at[1], swap_s.at[at], swap_r.at[at], mate)
        if p == pairs // 2:
            for plane in planes:
                landed(extras.at[plane, y, x], ez_r.at[plane])
            column = extras.at[:, y, x]
            for i, peer in enumerate(plane_peers):
                send(column, column, ep_s.at[i], ep_r.at[i], peer)
        if (p + 1) % (pairs // 2):
            continue
        q = p // (pairs // 2)
        cut = slice(q * part_rows, (q + 1) * part_rows)
        heads = []
        for h in range(head_count):
            part = slice(h * value_size, (h + 1) * value_size)
            retained = (
                inside[h][cut]
                + own[h][cut] * wide_values[cut, part]
                + carried[h][cut] * fades[h][cut]
            )
            heads.append(retained * inverse_rms(retained))
        if q == 0:
            need("out")
        mixer_out = mm(jnp.concatenate(heads, axis=1).astype(bf16), wo[...])
        residual = widened[cut] + mixer_out * inverse_rms(mixer_out)
        residuals.append(residual)
        gathered[z, y, x, cut] = (residual * inverse_rms(residual) * ffn_ref[...]).astype(bf16)
        block = piece(z, q)
        for k, peer in enumerate(z_peers):
            send(block, block, z_s.at[q, k], z_r.at[q, z], peer)
        spread(q, z)

    residual = jnp.concatenate(residuals, axis=0)
    normal_ffn = gathered[z, y, x]
    need("shared")
    hidden = (silu(mm(normal_ffn, sg[...])) * mm(normal_ffn, su[...])).astype(bf16)
    combined = mm(hidden, sd[...])
    gate = 1.0 / (1.0 + jnp.exp(-dense_ref[...]))

    for plane in planes:
        for q in range(2):
            landed(piece(plane, q), z_r.at[q, plane])
            spread(q, plane)
    for at, held in enumerate((eg, eu, ed, dg, du, dd)):
        landed(held.at[1], swap_r.at[at])
    for i in range(len(around)):
        landed(extras.at[:, behind(i)[0], behind(i)[1]], ep_r.at[i])

    def branches(at):
        for q in range(2):
            for i in range(len(around)):
                part = pl.ds(q * part_rows, part_rows)
                landed(gathered.at[at, behind(i)[0], behind(i)[1], part], d_r.at[q, at, i])
        count = ys * xs * seq_count
        inputs = gathered[at].reshape(count, width)
        scale = extras[at].reshape(count, extras.shape[-1]).astype(f32)
        place = lax.broadcasted_iota(jnp.int32, scale.shape, 1)
        dense = (
            silu(mm_t(inputs, dg[...].reshape(-1, width)))
            * mm_t(inputs, du[...].reshape(-1, width))
        ).astype(bf16)
        terms = gate * mm(dense, dd[...].reshape(-1, width))
        for slot, expert in enumerate((me, mate)):
            chosen = (place == expert) | (place == expert + expert_count)
            weight = jnp.sum(jnp.where(chosen, scale, 0.0), axis=1, keepdims=True)
            inner = (silu(mm(inputs, eg[slot])) * mm(inputs, eu[slot])).astype(bf16)
            terms = terms + weight * mm(inner, ed[slot])
        partial[at] = terms.astype(bf16).reshape(partial.shape[1:])
        for i, peer in enumerate(plane_peers):
            send(
                partial.at[at, beside(i)[0], beside(i)[1]],
                arrived.at[at, i],
                p_s.at[at, i],
                p_r.at[at, i],
                peer,
            )

    for at in range(zs):
        branches(at)

    def plane_sum(at):
        for i in range(len(around)):
            landed(arrived.at[at, i], p_r.at[at, i])
        value = partial[at, y, x].astype(f32)
        for i in range(len(around)):
            value = value + arrived[at, i].astype(f32)
        return value

    for k, peer in enumerate(z_peers):
        if k == zs - 2:
            combined = combined + plane_sum(z)
        summed[k] = plane_sum(planes[k]).astype(bf16)
        send(summed.at[k], returned.at[z], b_s.at[k], b_r.at[z], peer)
    if zs == 1:
        combined = combined + plane_sum(z)
    for plane in reversed(planes):
        landed(returned.at[plane], b_r.at[plane])
        combined = combined + returned[plane].astype(f32)
    out_ref[...] = (residual + combined * inverse_rms(combined)).astype(bf16)
    for copy in started:
        copy.wait_send()


def finish(a_ref, b_ref, c_ref, a_out, b_out, c_out, sems):
    copies = [
        pltpu.make_async_copy(origin, place, sems.at[at])
        for at, (origin, place) in enumerate([(a_ref, a_out), (b_ref, b_out), (c_ref, c_out)])
    ]
    for copy in copies:
        copy.start()
    for copy in copies:
        copy.wait()


def whole_layer(vectors, streams, shapes, dims, expert_count):
    seq_count, width, head_count, top_k = shapes
    zs, ys, xs = dims
    wq, wk, wv, wo, keys, values, state = streams[:7]
    experts, dense, shared = streams[7:10], streams[10:13], streams[13:16]
    z1, others = max(zs - 1, 1), max(ys * xs - 1, 1)
    extra = 2 * expert_count
    extra += -extra % lanes
    dma = pltpu.SemaphoreType.DMA
    vmem = pl.BlockSpec(memory_space=pltpu.VMEM)
    anywhere = pl.BlockSpec(memory_space=pl.ANY)
    grid = (zs, ys, xs, seq_count)
    scratch = [pltpu.VMEM(w.shape, w.dtype) for w in vectors + streams[:7]]
    scratch += [pltpu.VMEM((2,) + w.shape[1:], bf16) for w in experts]
    scratch += [pltpu.VMEM((2,) + w.shape, bf16) for w in dense]
    scratch += [pltpu.VMEM(w.shape, bf16) for w in shared]
    scratch += [
        pltpu.VMEM((head_count, seq_count, seq_count * keys.shape[1]), bf16),
        pltpu.VMEM((3, 8, lanes), f32),
        pltpu.VMEM(grid + (extra,), bf16),
        pltpu.VMEM(grid + (width,), bf16),
        pltpu.VMEM(grid + (width,), bf16),
        pltpu.VMEM((zs, others, seq_count, width), bf16),
        pltpu.VMEM((z1, seq_count, width), bf16),
        pltpu.VMEM((zs, seq_count, width), bf16),
    ]
    sems = [(9 * seq_count,), (6,), (6,)]
    sems += [(z1,), (zs,), (others,), (others,), (2, z1), (2, zs)]
    sems += [(2, zs, others)] * 2 + [(zs, others)] * 2 + [(z1,), (zs,)]
    out_shapes = [(seq_count, width), (seq_count, keys.shape[2]), (seq_count, values.shape[2])]
    results = pl.pallas_call(
        functools.partial(layer, dims, head_count, expert_count),
        out_shape=[pltpu.VMEM(shape, bf16) for shape in out_shapes],
        in_specs=[anywhere] * (len(vectors) + len(streams)),
        out_specs=[vmem] * 3,
        scratch_shapes=scratch + [dma(shape) for shape in sems],
        compiler_params=pltpu.CompilerParams(
            collective_id=0, has_side_effects=True, vmem_limit_bytes=58 * 1024 * 1024
        ),
    )(*vectors, *streams)
    return pl.pallas_call(
        finish,
        out_shape=[jax.ShapeDtypeStruct(shape, bf16) for shape in out_shapes],
        in_specs=[vmem] * 3,
        out_specs=[anywhere] * 3,
        scratch_shapes=[dma((3,))],
        compiler_params=pltpu.CompilerParams(vmem_limit_bytes=1024 * 1024),
    )(*results)


def per_device(
    tokens,
    lengths,
    cache_keys,
    cache_values,
    retention_state,
    mix_gain,
    query_weight,
    key_weight,
    value_weight,
    out_weight,
    ffn_gain,
    routes,
    route_scores,
    expert_gate,
    expert_up,
    expert_down,
    shared_gate,
    shared_up,
    shared_down,
    dense_gate,
    dense_up,
    dense_down,
    dense_mix,
):
    device_count = lax.axis_size("ep")
    expert_count = device_count * expert_gate.shape[0]
    seq_count, width = tokens.shape
    vectors = (
        tokens,
        lengths.reshape(1, seq_count),
        routes.T,
        route_scores.T,
        mix_gain.reshape(1, width),
        ffn_gain.reshape(1, width),
        dense_mix.reshape(1, width),
    )
    streams = (
        query_weight,
        key_weight,
        value_weight,
        out_weight,
        cache_keys,
        cache_values,
        retention_state,
        expert_gate,
        expert_up,
        expert_down,
        dense_gate,
        dense_up,
        dense_down,
        shared_gate,
        shared_up,
        shared_down,
    )
    shapes = (seq_count, width, retention_state.shape[1], routes.shape[1])
    return tuple(
        whole_layer(vectors, streams, shapes, slice_dims(device_count), expert_count)
    )


def solution(mesh):
    in_specs = (
        P("ep", None),
        P("ep"),
        P("ep", None, None),
        P("ep", None, None),
        P("ep", None, None, None),
        P(),
        P(),
        P(),
        P(),
        P(),
        P(),
        P("ep", None),
        P("ep", None),
        P("ep", None, None),
        P("ep", None, None),
        P("ep", None, None),
        P(),
        P(),
        P(),
        P("ep", None),
        P("ep", None),
        P("ep", None),
        P(),
    )
    out_specs = (P("ep", None), P("ep", None), P("ep", None))
    return jax.shard_map(
        per_device, mesh=mesh, in_specs=in_specs, out_specs=out_specs, check_vma=False
    )
```

```python
import functools
import math

import jax
import jax.numpy as jnp
from jax import lax
from jax.experimental import pallas as pl
from jax.experimental.pallas import tpu as pltpu
from jax.sharding import PartitionSpec as P

eps = 1e-06
route_scale = 2.5
rope_base = 10000.0

f32 = jnp.float32
bf16 = jnp.bfloat16
lanes = 128


def inverse_rms(values):
    return lax.rsqrt(jnp.mean(values * values, axis=-1, keepdims=True) + eps)


def mm(a, b):
    return lax.dot_general(a, b, (((1,), (0,)), ((), ())), preferred_element_type=f32)


def mm_t(a, b):
    return lax.dot_general(a, b, (((1,), (1,)), ((), ())), preferred_element_type=f32)


def cos_sin(angles):
    turn = jnp.floor(angles * (2.0 / math.pi) + 0.5)
    r = angles - turn * 1.5703125
    r = r - turn * 4.837512969970703125e-4
    r = r - turn * 7.54978995489188216e-8
    z = r * r
    sine = ((-1.9515295891e-4 * z + 8.3321608736e-3) * z - 1.6666654611e-1) * z * r + r
    cosine = ((2.443315711809948e-5 * z - 1.388731625493765e-3) * z + 4.166664568298827e-2) * z * z
    cosine = cosine - 0.5 * z + 1.0
    quarter = turn - 4.0 * jnp.floor(turn * 0.25)
    odd = (quarter == 1.0) | (quarter == 3.0)
    c = jnp.where(odd, sine, cosine)
    s = jnp.where(odd, cosine, sine)
    c = jnp.where((quarter == 1.0) | (quarter == 2.0), -c, c)
    s = jnp.where(quarter >= 2.0, -s, s)
    return c, s


def to_columns(row, count):
    return jnp.transpose(jnp.broadcast_to(row, (lanes, lanes)))[0:count]


def route_block(routes, weight, top_k, expert_count, wide, count):
    tiles = []
    for at in range(0, wide, lanes):
        place = at + lax.broadcasted_iota(jnp.int32, (lanes, lanes), 0)
        lower = place >= expert_count
        expert = jnp.where(lower, place - expert_count, place)
        named = jnp.zeros((lanes, lanes), f32)
        for k in range(top_k):
            named = named + jnp.where(expert == routes[k : k + 1], weight[k : k + 1], 0.0)
        upper = named.astype(bf16).astype(f32)
        kept = jnp.where(lower, named - upper, upper)
        tiles.append(jnp.transpose(kept)[0:count].astype(bf16))
    return tiles


def silu(v):
    return v / (1.0 + jnp.exp(-v))


def slice_dims(device_count):
    side = max(1, math.isqrt(device_count // 8))
    return device_count // (2 * side * side), side, side


def layer(
    dims,
    head_count,
    expert_count,
    tokens_hbm,
    lengths_hbm,
    routes_hbm,
    scores_hbm,
    mix_hbm,
    ffn_hbm,
    dense_hbm,
    wq_hbm,
    wk_hbm,
    wv_hbm,
    wo_hbm,
    keys_hbm,
    values_hbm,
    state_hbm,
    eg_hbm,
    eu_hbm,
    ed_hbm,
    dg_hbm,
    du_hbm,
    dd_hbm,
    sg_hbm,
    su_hbm,
    sd_hbm,
    out_ref,
    new_keys_ref,
    new_values_ref,
    tokens_ref,
    lengths_ref,
    routes_ref,
    scores_ref,
    mix_ref,
    ffn_ref,
    dense_ref,
    wq,
    wk,
    wv,
    wo,
    keys,
    values,
    state,
    eg,
    eu,
    ed,
    dg,
    du,
    dd,
    sg,
    su,
    sd,
    weights,
    small,
    extras,
    gathered,
    partial,
    arrived,
    summed,
    returned,
    total,
    l_sem,
    swap_s,
    swap_r,
    ez_s,
    ez_r,
    ep_s,
    ep_r,
    z_s,
    z_r,
    d_s,
    d_r,
    p_s,
    p_r,
    b_s,
    b_r,
):
    seq_count, block_size, key_width = keys.shape
    key_size = key_width // head_count
    width = tokens_ref.shape[1]
    value_width = values.shape[2]
    value_size = value_width // head_count
    pairs = seq_count // 2

    zs, ys, xs = dims
    me = lax.axis_index("ep")
    core = lax.rem(me, 2)
    x = lax.rem(me // 2, xs)
    y = lax.rem(me // (2 * xs), ys)
    z = me // (2 * xs * ys)

    def device(zz, yy, xx, cc):
        return ((zz * ys + yy) * xs + xx) * 2 + cc

    planes = [k + (k - z + zs) // zs for k in range(zs - 1)]
    around = sorted(
        ((dy, dx) for dy in range(ys) for dx in range(xs) if dy or dx),
        key=lambda step: -min(step[0], ys - step[0]) - min(step[1], xs - step[1]),
    )

    def beside(i):
        dy, dx = around[i]
        return lax.rem(y + dy, ys), lax.rem(x + dx, xs)

    def behind(i):
        dy, dx = around[i]
        return lax.rem(y - dy + ys, ys), lax.rem(x - dx + xs, xs)

    mate = device(z, y, x, 1 - core)
    direct = zs > 2
    last = zs - 1
    far = last - z
    at_end = (z == 0) | (z == last)

    def unless(condition, action):
        if direct:
            pl.when(jnp.logical_not(condition))(action)
        else:
            action()

    z_peers = [device(plane, y, x, core) for plane in planes]
    plane_peers = [device(z, *beside(i), core) for i in range(len(around))]

    waiting = []

    def plan(name, origin, place, pieces=1):
        count = origin.shape[0] // pieces
        for at in range(pieces):
            part = pl.ds(at * count, count)
            index = len(waiting)
            copy = pltpu.make_async_copy(origin.at[part], place.at[part], l_sem.at[index])
            waiting.append((name, copy))

    plan("tokens", tokens_hbm, tokens_ref)
    plan("tokens", mix_hbm, mix_ref)
    plan("query", wq_hbm, wq, 2)
    plan("small", lengths_hbm, lengths_ref)
    plan("small", routes_hbm, routes_ref)
    plan("small", scores_hbm, scores_ref)
    plan("key", wk_hbm, wk, 2)
    for p in range(0, pairs, 2):
        part = pl.ds(2 * p, 4)
        plan(("keys", p), keys_hbm.at[part], keys.at[part])
    plan("value", wv_hbm, wv, 4)
    for p in range(pairs):
        part = pl.ds(2 * p, 2)
        plan(("values", p), values_hbm.at[part], values.at[part])
        plan(("state", p), state_hbm.at[part], state.at[part], 2)
        if p == 0:
            plan("swap", eg_hbm, eg.at[pl.ds(0, 1)])
            plan("swap", eu_hbm, eu.at[pl.ds(0, 1)])
            plan("swap", ed_hbm, ed.at[pl.ds(0, 1)])
            plan("swap", dg_hbm, dg.at[0])
            plan("swap", du_hbm, du.at[0])
            plan("swap", dd_hbm, dd.at[0])
        if p == pairs // 2 - 1:
            plan("out", wo_hbm, wo, 4)
            plan("out", ffn_hbm, ffn_ref)
    plan("shared", sg_hbm, sg)
    plan("shared", su_hbm, su)
    plan("shared", sd_hbm, sd)
    plan("shared", dense_hbm, dense_ref)

    def swap_loads():
        for label, copy in waiting:
            if label == "swap":
                copy.start()

    before = None
    for label, copy in waiting:
        if label == "swap" and before != "swap":
            pl.when(core == 1)(swap_loads)
        if label == "shared" and before != "shared":
            pl.when(core == 0)(swap_loads)
        before = label
        if label != "swap":
            copy.start()

    def need(name):
        for label, copy in waiting:
            if label == name:
                copy.wait()

    barrier = pltpu.get_barrier_semaphore()
    peers = z_peers + plane_peers + [mate]
    peers += [device(plane, *beside(i), core) for plane in planes for i in range(len(around))]
    for peer in peers:
        pl.semaphore_signal(
            barrier, inc=1, device_id=(peer,), device_id_type=pl.DeviceIdType.MESH
        )

    started = []

    def drained(place, sem):
        pltpu.make_async_remote_copy(
            src_ref=place,
            dst_ref=place,
            send_sem=sem,
            recv_sem=sem,
            device_id=(mate,),
            device_id_type=pl.DeviceIdType.MESH,
        ).wait_send()

    def launch(origin, place, send_sem, recv_sem, peer):
        pltpu.make_async_remote_copy(
            src_ref=origin,
            dst_ref=place,
            send_sem=send_sem,
            recv_sem=recv_sem,
            device_id=(peer,),
            device_id_type=pl.DeviceIdType.MESH,
        ).start()

    def send(origin, place, send_sem, recv_sem, peer):
        copy = pltpu.make_async_remote_copy(
            src_ref=origin,
            dst_ref=place,
            send_sem=send_sem,
            recv_sem=recv_sem,
            device_id=(peer,),
            device_id_type=pl.DeviceIdType.MESH,
        )
        copy.start()
        started.append(copy)

    def landed(place, sem):
        pltpu.make_async_remote_copy(
            src_ref=place,
            dst_ref=place,
            send_sem=sem,
            recv_sem=sem,
            device_id=(mate,),
            device_id_type=pl.DeviceIdType.MESH,
        ).wait_recv()

    need("tokens")
    widened = tokens_ref[...].astype(f32)
    normal_in = (widened * inverse_rms(widened) * mix_ref[...]).astype(bf16)

    need("small")
    top_k = routes_ref.shape[0]
    small[...] = jnp.zeros_like(small)
    small[0, 0:1, 0:seq_count] = lengths_ref[...].astype(f32)
    small[1, 0:top_k, 0:seq_count] = routes_ref[...].astype(f32)
    scores = scores_ref[...]
    small[2, 0:top_k, 0:seq_count] = (
        scores / jnp.sum(scores, axis=0, keepdims=True) * route_scale
    )
    tiles = route_block(
        small[1].astype(jnp.int32),
        small[2],
        top_k,
        expert_count,
        extras.shape[-1],
        seq_count,
    )
    for at, tile in enumerate(tiles):
        extras[z, y, x, :, at * lanes : (at + 1) * lanes] = tile

    positions = to_columns(small[0, 0:1], seq_count)
    lane = lax.broadcasted_iota(jnp.int32, (seq_count, lanes), 1)
    row = lax.broadcasted_iota(jnp.int32, (seq_count, lanes), 0)
    half = key_size // 2
    entry = jnp.where(lane < half, lane, lane - half).astype(f32)
    inverse = jnp.exp(entry * (-math.log(rope_base) / half))
    cosine, sine = cos_sin(positions * inverse)
    signed = jnp.where(lane < half, -sine, sine)
    filled = positions - block_size * jnp.floor(positions * (1.0 / block_size))
    distance = filled - lane.astype(f32)
    live = distance > 0.0
    rates = [math.log1p(-(2.0 ** (-5 - h))) for h in range(head_count)]
    decay = [
        jnp.where(live, jnp.exp(jnp.maximum(distance, 0.0) * rate), 0.0) for rate in rates
    ]

    def rotated(raw):
        return raw * cosine + pltpu.roll(raw, half, 1) * signed

    need("query")
    raw_query = mm(normal_in, wq[...])
    need("key")
    raw_key = mm(normal_in, wk[...])
    queries, own = [], []
    for h in range(head_count):
        part = slice(h * key_size, (h + 1) * key_size)
        query = (rotated(raw_query[:, part]) * key_size ** (-0.5)).astype(bf16)
        key = rotated(raw_key[:, part]).astype(bf16)
        new_keys_ref[:, part] = key
        queries.append(query)
        weight = jnp.sum(query.astype(f32) * key.astype(f32), axis=1, keepdims=True)
        own.append(weight.astype(bf16).astype(f32))


    rows = 2 * block_size
    for p in range(pairs):
        if p % 2 == 0:
            need(("keys", p))
        for h in range(head_count):
            stored = keys[2 * p : 2 * p + 2, :, h * key_size : (h + 1) * key_size]
            scores = mm_t(queries[h], stored.reshape(rows, key_size))
            for i in range(2):
                part = scores[:, i * block_size : (i + 1) * block_size] * decay[h]
                weights[h, :, p * rows + i * block_size : p * rows + (i + 1) * block_size] = (
                    jnp.where(row == 2 * p + i, part, 0.0).astype(bf16)
                )

    need("value")
    new_values = mm(normal_in, wv[...]).astype(bf16)
    new_values_ref[...] = new_values

    wide_values = new_values.astype(f32)
    inside = [jnp.zeros((seq_count, value_size), f32) for _ in range(head_count)]
    carried = [jnp.zeros((seq_count, value_size), f32) for _ in range(head_count)]
    fades = [jnp.exp((filled[:, 0:1] + 1.0) * rate) for rate in rates]
    residuals = []

    def swap_copies():
        return [
            pltpu.make_async_remote_copy(
                src_ref=held.at[0],
                dst_ref=held.at[1],
                send_sem=swap_s.at[at],
                recv_sem=swap_r.at[at],
                device_id=(mate,),
                device_id_type=pl.DeviceIdType.MESH,
            )
            for at, held in enumerate((eg, eu, ed, dg, du, dd))
        ]

    def swap_weights():
        need("swap")
        for copy in swap_copies():
            copy.start()

    part_rows = seq_count // 2

    def piece(at, q):
        return gathered.at[at, y, x, pl.ds(q * part_rows, part_rows)]

    def spread(q, at):
        part = piece(at, q)
        for i, peer in enumerate(plane_peers):
            launch(part, part, d_s.at[q, at, i], d_r.at[q, at, i], peer)

    for p in range(pairs):
        need(("values", p))
        for h in range(head_count):
            stored = values[2 * p : 2 * p + 2, :, h * value_size : (h + 1) * value_size]
            inside[h] = inside[h] + mm(
                weights[h, :, p * rows : (p + 1) * rows], stored.reshape(rows, value_size)
            )
        need(("state", p))
        for h in range(head_count):
            chosen = jnp.concatenate(
                [jnp.where(row == 2 * p + i, queries[h].astype(f32), 0.0) for i in range(2)],
                axis=1,
            ).astype(bf16)
            held = state[2 * p : 2 * p + 2, h].reshape(2 * key_size, value_size)
            carried[h] = carried[h] + mm(chosen, held.astype(bf16))
        if p == 1:
            pl.semaphore_wait(barrier, len(peers))
            mine = extras.at[z, y, x]
            for k, peer in enumerate(z_peers):
                send(mine, mine, ez_s.at[k], ez_r.at[z], peer)
            pl.when(core == 1)(swap_weights)
        if (p + 1) % (pairs // 2):
            continue
        q = p // (pairs // 2)
        cut = slice(q * part_rows, (q + 1) * part_rows)
        heads = []
        for h in range(head_count):
            part = slice(h * value_size, (h + 1) * value_size)
            retained = (
                inside[h][cut]
                + own[h][cut] * wide_values[cut, part]
                + carried[h][cut] * fades[h][cut]
            )
            heads.append(retained * inverse_rms(retained))
        if q == 0:
            need("out")
        mixer_out = mm(jnp.concatenate(heads, axis=1).astype(bf16), wo[...])
        residual = widened[cut] + mixer_out * inverse_rms(mixer_out)
        residuals.append(residual)
        gathered[z, y, x, cut] = (residual * inverse_rms(residual) * ffn_ref[...]).astype(bf16)
        block = piece(z, q)
        for k, peer in enumerate(z_peers):
            send(block, block, z_s.at[q, k], z_r.at[q, z], peer)
        spread(q, z)

    pl.when(core == 0)(swap_weights)
    for plane in planes:
        landed(extras.at[plane, y, x], ez_r.at[plane])
    column = extras.at[:, y, x]
    for i, peer in enumerate(plane_peers):
        send(column, column, ep_s.at[i], ep_r.at[i], peer)
    residual = jnp.concatenate(residuals, axis=0)
    normal_ffn = gathered[z, y, x]
    def forward(k):
        def onward():
            for q in range(2):
                landed(piece(planes[k], q), z_r.at[q, planes[k]])
                spread(q, planes[k])

        onward()

    for k in range(0, max(zs - 2, min(1, zs - 1))):
        forward(k)
    need("shared")
    hidden = (silu(mm(normal_ffn, sg[...])) * mm(normal_ffn, su[...])).astype(bf16)
    combined = mm(hidden, sd[...])
    gate = 1.0 / (1.0 + jnp.exp(-dense_ref[...]))

    if zs > 2:
        forward(zs - 2)

    for at, held in enumerate((eg, eu, ed, dg, du, dd)):
        landed(held.at[1], swap_r.at[at])
    for i in range(len(around)):
        landed(extras.at[:, behind(i)[0], behind(i)[1]], ep_r.at[i])

    def branches(at):
        for q in range(2):
            for i in range(len(around)):
                part = pl.ds(q * part_rows, part_rows)
                landed(gathered.at[at, behind(i)[0], behind(i)[1], part], d_r.at[q, at, i])
        count = ys * xs * seq_count
        inputs = gathered[at].reshape(count, width)
        scale = extras[at].reshape(count, extras.shape[-1]).astype(f32)
        place = lax.broadcasted_iota(jnp.int32, scale.shape, 1)
        dense = (
            silu(mm_t(inputs, dg[...].reshape(-1, width)))
            * mm_t(inputs, du[...].reshape(-1, width))
        ).astype(bf16)
        terms = gate * mm(dense, dd[...].reshape(-1, width))
        for slot, expert in enumerate((me, mate)):
            chosen = (place == expert) | (place == expert + expert_count)
            weight = jnp.sum(jnp.where(chosen, scale, 0.0), axis=1, keepdims=True)
            inner = (silu(mm(inputs, eg[slot])) * mm(inputs, eu[slot])).astype(bf16)
            terms = terms + weight * mm(inner, ed[slot])
        partial[at] = terms.astype(bf16).reshape(partial.shape[1:])

        def in_plane():
            for i, peer in enumerate(plane_peers):
                launch(
                    partial.at[at, beside(i)[0], beside(i)[1]],
                    arrived.at[at, i],
                    p_s.at[at, i],
                    p_r.at[at, i],
                    peer,
                )

        def straight():
            for i in range(len(around)):
                launch(
                    partial.at[at, beside(i)[0], beside(i)[1]],
                    arrived.at[z, i],
                    p_s.at[at, i],
                    p_r.at[z, i],
                    device(at, *beside(i), core),
                )
            launch(
                partial.at[at, y, x],
                returned.at[z],
                b_s.at[0 if at == 0 else zs - 2],
                b_r.at[z],
                device(at, y, x, core),
            )

        if direct and at in (0, last):
            pl.when(z == last - at)(straight)
            unless(z == last - at, in_plane)
        else:
            in_plane()

    for at in range(zs):
        branches(at)

    def plane_sum(at):
        for i in range(len(around)):
            landed(arrived.at[at, i], p_r.at[at, i])
        value = partial[at, y, x].astype(f32)
        for i in range(len(around)):
            value = value + arrived[at, i].astype(f32)
        return value

    def homeward(k):
        summed[k] = plane_sum(planes[k]).astype(bf16)
        launch(summed.at[k], returned.at[z], b_s.at[k], b_r.at[z], z_peers[k])

    for k in range(zs - 1):
        if k == 0:
            unless(z == last, functools.partial(homeward, k))
        elif k == zs - 2:
            unless(z == 0, functools.partial(homeward, k))
        else:
            homeward(k)
    total[...] = combined + plane_sum(z)

    def far_sum():
        value = total[...]
        for i in range(len(around)):
            landed(arrived.at[far, i], p_r.at[far, i])
            value = value + arrived[far, i].astype(f32)
        total[...] = value

    if direct:
        pl.when(at_end)(far_sum)
    combined = total[...]
    for plane in reversed(planes):
        landed(returned.at[plane], b_r.at[plane])
        combined = combined + returned[plane].astype(f32)
    out_ref[...] = (residual + combined * inverse_rms(combined)).astype(bf16)
    for copy in started + swap_copies():
        copy.wait_send()
    for at in range(zs):
        for i in range(len(around)):
            drained(partial.at[at, y, x], p_s.at[at, i])
            for q in range(2):
                drained(piece(at, q), d_s.at[q, at, i])
    for k in range(zs - 1):
        drained(partial.at[0, y, x], b_s.at[k])


def finish(a_ref, b_ref, c_ref, a_out, b_out, c_out, sems):
    copies = [
        pltpu.make_async_copy(origin, place, sems.at[at])
        for at, (origin, place) in enumerate([(a_ref, a_out), (b_ref, b_out), (c_ref, c_out)])
    ]
    for copy in copies:
        copy.start()
    for copy in copies:
        copy.wait()


def whole_layer(vectors, streams, shapes, dims, expert_count):
    seq_count, width, head_count, top_k = shapes
    zs, ys, xs = dims
    wq, wk, wv, wo, keys, values, state = streams[:7]
    experts, dense, shared = streams[7:10], streams[10:13], streams[13:16]
    z1, others = max(zs - 1, 1), max(ys * xs - 1, 1)
    extra = 2 * expert_count
    extra += -extra % lanes
    dma = pltpu.SemaphoreType.DMA
    vmem = pl.BlockSpec(memory_space=pltpu.VMEM)
    anywhere = pl.BlockSpec(memory_space=pl.ANY)
    grid = (zs, ys, xs, seq_count)
    scratch = [pltpu.VMEM(w.shape, w.dtype) for w in vectors + streams[:7]]
    scratch += [pltpu.VMEM((2,) + w.shape[1:], bf16) for w in experts]
    scratch += [pltpu.VMEM((2,) + w.shape, bf16) for w in dense]
    scratch += [pltpu.VMEM(w.shape, bf16) for w in shared]
    scratch += [
        pltpu.VMEM((head_count, seq_count, seq_count * keys.shape[1]), bf16),
        pltpu.VMEM((3, 8, lanes), f32),
        pltpu.VMEM(grid + (extra,), bf16),
        pltpu.VMEM(grid + (width,), bf16),
        pltpu.VMEM(grid + (width,), bf16),
        pltpu.VMEM((zs, others, seq_count, width), bf16),
        pltpu.VMEM((z1, seq_count, width), bf16),
        pltpu.VMEM((zs, seq_count, width), bf16),
        pltpu.VMEM((seq_count, width), f32),
    ]
    sems = [(9 * seq_count,), (6,), (6,)]
    sems += [(z1,), (zs,), (others,), (others,), (2, z1), (2, zs)]
    sems += [(2, zs, others)] * 2 + [(zs, others)] * 2 + [(z1,), (zs,)]
    out_shapes = [(seq_count, width), (seq_count, keys.shape[2]), (seq_count, values.shape[2])]
    results = pl.pallas_call(
        functools.partial(layer, dims, head_count, expert_count),
        out_shape=[pltpu.VMEM(shape, bf16) for shape in out_shapes],
        in_specs=[anywhere] * (len(vectors) + len(streams)),
        out_specs=[vmem] * 3,
        scratch_shapes=scratch + [dma(shape) for shape in sems],
        compiler_params=pltpu.CompilerParams(
            collective_id=0, has_side_effects=True, vmem_limit_bytes=58 * 1024 * 1024
        ),
    )(*vectors, *streams)
    return pl.pallas_call(
        finish,
        out_shape=[jax.ShapeDtypeStruct(shape, bf16) for shape in out_shapes],
        in_specs=[vmem] * 3,
        out_specs=[anywhere] * 3,
        scratch_shapes=[dma((3,))],
        compiler_params=pltpu.CompilerParams(vmem_limit_bytes=1024 * 1024),
    )(*results)


def per_device(
    tokens,
    lengths,
    cache_keys,
    cache_values,
    retention_state,
    mix_gain,
    query_weight,
    key_weight,
    value_weight,
    out_weight,
    ffn_gain,
    routes,
    route_scores,
    expert_gate,
    expert_up,
    expert_down,
    shared_gate,
    shared_up,
    shared_down,
    dense_gate,
    dense_up,
    dense_down,
    dense_mix,
):
    device_count = lax.axis_size("ep")
    expert_count = device_count * expert_gate.shape[0]
    seq_count, width = tokens.shape
    vectors = (
        tokens,
        lengths.reshape(1, seq_count),
        routes.T,
        route_scores.T,
        mix_gain.reshape(1, width),
        ffn_gain.reshape(1, width),
        dense_mix.reshape(1, width),
    )
    streams = (
        query_weight,
        key_weight,
        value_weight,
        out_weight,
        cache_keys,
        cache_values,
        retention_state,
        expert_gate,
        expert_up,
        expert_down,
        dense_gate,
        dense_up,
        dense_down,
        shared_gate,
        shared_up,
        shared_down,
    )
    shapes = (seq_count, width, retention_state.shape[1], routes.shape[1])
    return tuple(
        whole_layer(vectors, streams, shapes, slice_dims(device_count), expert_count)
    )


def solution(mesh):
    in_specs = (
        P("ep", None),
        P("ep"),
        P("ep", None, None),
        P("ep", None, None),
        P("ep", None, None, None),
        P(),
        P(),
        P(),
        P(),
        P(),
        P(),
        P("ep", None),
        P("ep", None),
        P("ep", None, None),
        P("ep", None, None),
        P("ep", None, None),
        P(),
        P(),
        P(),
        P("ep", None),
        P("ep", None),
        P("ep", None),
        P(),
    )
    out_specs = (P("ep", None), P("ep", None), P("ep", None))
    return jax.shard_map(
        per_device, mesh=mesh, in_specs=in_specs, out_specs=out_specs, check_vma=False
    )
```
